128 devices in a mesh: ep: 64 (over z, y, x), tp: 2 (over core).
Axes of the slice: x: 4, y: 4, z: 4, core: 2. Of those that a mesh axis runs over, the one named last changes fastest.
Arguments:
- stream: bfloat16 [4096, 2048], P('ep', 'tp'), may hold values from -40 to 40
- conv_state: bfloat16 [4096, 3, 2048], P('ep', None, 'tp'), may hold values from -5 to 5
- recur_state: float32 [4096, 2048], P('ep', 'tp'), may hold values from -5 to 5
- mix_gain: float32 [2048], replicated, may hold values from 0.1 to 1.9
- branch_weight: bfloat16 [2048, 2048], P(None, 'tp'), may hold values from -0.125 to 0.125
- gate_weight: bfloat16 [2048, 2048], P(None, 'tp'), may hold values from -0.125 to 0.125
- conv_taps: float32 [4, 2048], P(None, 'tp'), may hold values from -3 to 3
- recur_map: bfloat16 [16, 128, 128], P('tp'), may hold values from -0.5 to 0.5
- input_map: bfloat16 [16, 128, 128], P('tp'), may hold values from -0.5 to 0.5
- decay_logit: float32 [2048], P('tp'), may hold values from -1 to 6
- out_weight: bfloat16 [2048, 2048], P(None, 'tp'), may hold values from -0.125 to 0.125
- moe_gain: float32 [2048], replicated, may hold values from 0.1 to 1.9
- route_ids: int32 [4096, 6], P('ep'), may hold values from 0 to 63, all different within a row; in each aligned block of 64 rows (0 to 63, 64 to 127, ...) at most 18 rows name the same one
- route_weights: float32 [4096, 6], P('ep'), may hold values from 0.2 to 1
- expert_gate: bfloat16 [64, 2048, 512], P('ep', None, 'tp'), may hold values from -0.125 to 0.125
- expert_up: bfloat16 [64, 2048, 512], P('ep', None, 'tp'), may hold values from -0.125 to 0.125
- expert_down: bfloat16 [64, 512, 2048], P('ep', None, 'tp'), may hold values from -0.25 to 0.25
- dense_gate: bfloat16 [2048, 512], P(None, 'tp'), may hold values from -0.125 to 0.125
- dense_up: bfloat16 [2048, 512], P(None, 'tp'), may hold values from -0.125 to 0.125
- dense_down: bfloat16 [512, 2048], P(None, 'tp'), may hold values from -0.25 to 0.25
- dense_scale: float32 [2048], P('tp'), may hold values from 0.1 to 1.9
Outputs:
- result: bfloat16 [4096, 2048], P('ep', 'tp')
- new_state: float32 [4096, 2048], P('ep', 'tp')
- new_conv: bfloat16 [4096, 3, 2048], P('ep', None, 'tp')
The draws below stay inside these ranges and needn't reach their ends.
Inputs may be any that keep to these rules, and one draw needn't show every extreme that they name: `route_ids`: each row names 6 different experts; among the rows of one index of ep no expert is named by more than 18 rows, and in every draw some expert is named by exactly 18 rows of some index.
All inputs are finite; a program needn't handle non-finite values.
Results may differ from the reference program's by a relative error of at most 0.014.
Values may be sent and summed in bfloat16 or wider, within the bound.
No kernel may reach another device: no remote copies, remote signals or barrier semaphores. Data moves between devices by JAX's collectives and lax.ppermute only.
A program may use at most 128 MiB of HBM per device.

```python
import math
import jax
import jax.numpy as jnp
import numpy as np
from jax import lax

D = 2048
W = 2048
LBLK = 16
BLK = 128
FFE = 512
FFS = 512
TOP = 6
SEQ_DEV = 64
BATCH = 4096
EXPERTS = 64
CAP = 18
N_EP = 64


def draw_stream(key, part):
    key_cols, key_rows, key_base = jax.random.split(key, 3)
    positions = jnp.arange(D, dtype=jnp.float32) / D
    rough = jnp.exp(jax.random.uniform(key_cols, (D,), jnp.float32, -0.7, 0.7))
    row_scale = jnp.exp(jax.random.uniform(key_rows, (BATCH, 1), jnp.float32, jnp.log(0.5), jnp.log(2.5)))
    column_scale = jnp.exp(jnp.log(3.0) * (positions - 0.5)) * rough
    base = jnp.clip(jax.random.normal(key_base, (BATCH, D), jnp.float32), -4.0, 4.0)
    return (base * column_scale[None, :] * row_scale).astype(jnp.bfloat16)


def levels(rng, shape, cuts, least, high):
    def one(dim, shards_of):
        heights = jax.random.uniform(jax.random.fold_in(jax.random.fold_in(rng, 6), dim), (shards_of,), jnp.float32, least / len(cuts), high / len(cuts))
        return jnp.repeat(jnp.exp(heights), shape[dim] // shards_of).reshape((-1,) + (1,) * (len(shape) - dim - 1))

    level = one(*cuts[0])
    for cut in cuts[1:]:
        level = level * one(*cut)
    return level


def routed_block(key, own, number, rows, count, top, bound, skew):
    order = jax.random.permutation(key, count)
    heavy_load, common = portions_of(count, rows * top, bound, skew, True), portions_of(count, rows * top, bound, skew, False)
    places = jnp.arange(count)

    def named(lengths, offset_by):
        used = int((lengths > 0).sum())
        fixed = max(1, used // 4)
        moved = fixed + (places - fixed + offset_by * (used - fixed)) % max(1, count - fixed)
        return jnp.zeros((count,), jnp.int32).at[order[jnp.where(places < fixed, places, moved)]].set(jnp.asarray(lengths, jnp.int32))

    lengths = jnp.where(number % 4 == 0, named(heavy_load, number // 4), named(common, number - number // 4 - 1))
    mixed = jax.random.permutation(jax.random.fold_in(own, 3), count)
    source_of, taker = mixed[0:count // 2 * 2:2], mixed[1:count // 2 * 2:2]
    slack = jnp.minimum(lengths[source_of] - 1, bound - lengths[taker]) // 2
    slack = jnp.where((source_of == order[0]) | (taker == order[0]) | (lengths[taker] == 0), 0, jnp.maximum(slack, 0))
    moved = jax.random.randint(jax.random.fold_in(own, 4), (count // 2,), 0, 1 << 20) % (slack + 1)
    lengths = lengths.at[source_of].add(-moved).at[taker].add(moved)
    labels = jnp.searchsorted(jnp.cumsum(lengths), jnp.arange(rows * top), side="right").astype(jnp.int32)
    listing = labels.reshape(top, rows).T
    listing = listing[jax.random.permutation(jax.random.fold_in(own, 1), rows)]
    offset_by = jax.random.randint(jax.random.fold_in(own, 2), (rows, 1), 0, top)
    return jnp.take_along_axis(listing, (jnp.arange(top)[None, :] + offset_by) % top, axis=1)


def portions_of(amount, total, limit, lean, full):
    portions = [(1 << 20) // math.isqrt(grade ** lean) + 1 for grade in range(1, amount + 1)]
    largest = limit if full else min(limit, max(-(-total // amount), total * portions[0] // sum(portions)))
    least = 1 if total - largest >= amount - 1 else 0
    counts, surplus = [largest] + [least] * (amount - 1), total - largest - least * (amount - 1)
    while surplus > 0:
        free = [i for i in range(1, amount) if counts[i] < largest] or [i for i in range(1, amount) if counts[i] < limit]
        mass, remaining = sum([portions[i] for i in free]), surplus
        for i in free:
            addition = min(limit - counts[i], max(1, remaining * portions[i] // mass), surplus)
            counts[i] = counts[i] + addition
            surplus = surplus - addition
    return np.array(counts)


def noise(stream_key, shape, spread, limit, cuts=(), kind=jnp.bfloat16):
    array = spread * jax.random.normal(stream_key, shape, jnp.float32)
    if cuts:
        array = array * levels(stream_key, shape, cuts, -0.22, 0.18)
    return jnp.clip(array, -limit, limit).astype(kind)


def setup_inputs(seed: int = 0) -> dict:
    arg_keys = jax.random.split(jax.random.key(seed), 22)
    stream = draw_stream(jax.random.fold_in(arg_keys[21], 71), 0)
    conv_state = noise(arg_keys[1], (BATCH, 3, W), 1.0, 5.0, ((0, 64), (2, 2)))
    recur_state = noise(arg_keys[2], (BATCH, W), 1.0, 5.0, ((0, 64), (1, 2)), jnp.float32)
    mix_gain = jnp.clip(1.0 + 0.18 * jax.random.normal(arg_keys[3], (D,), jnp.float32), 0.1, 1.9)
    branch_weight = noise(arg_keys[4], (D, W), D ** -0.5, 0.125, ((1, 2),))
    gate_weight = noise(arg_keys[5], (D, W), D ** -0.5, 0.125, ((1, 2),))
    conv_taps = noise(arg_keys[6], (4, W), 0.5, 3.0, ((1, 2),), jnp.float32)
    recur_map = noise(arg_keys[7], (LBLK, BLK, BLK), BLK ** -0.5, 0.5, ((0, 2),))
    input_map = noise(arg_keys[8], (LBLK, BLK, BLK), BLK ** -0.5, 0.5, ((0, 2),))
    decay_logit = jnp.clip(-1.0 + 7.0 * jax.random.uniform(arg_keys[9], (W,), jnp.float32) ** levels(arg_keys[9], (W,), ((0, 2),), -0.2, 0.2), -1.0, 6.0)
    out_weight = noise(arg_keys[10], (W, D), W ** -0.5, 0.125, ((1, 2),))
    moe_gain = jnp.clip(1.0 + 0.18 * jax.random.normal(arg_keys[11], (D,), jnp.float32), 0.1, 1.9)
    route_ids_keys = jax.random.split(jax.random.fold_in(arg_keys[12], 1), BATCH // SEQ_DEV)
    route_ids_turns = jax.random.permutation(jax.random.fold_in(arg_keys[12], 3), BATCH // SEQ_DEV)
    route_ids = jax.vmap(lambda own, number: routed_block(jax.random.fold_in(arg_keys[12], 2), own, number, SEQ_DEV, EXPERTS, TOP, CAP, 1))(route_ids_keys, route_ids_turns).reshape((BATCH, TOP))
    route_weights = jnp.clip(0.2 + 0.8 * jax.random.uniform(arg_keys[13], (BATCH, TOP), jnp.float32) ** levels(arg_keys[13], (BATCH, TOP), ((0, 64),), -0.2, 0.2), 0.2, 1.0)
    expert_gate = noise(arg_keys[14], (EXPERTS, D, FFE), D ** -0.5, 0.125, ((0, 64), (2, 2)))
    expert_up = noise(arg_keys[15], (EXPERTS, D, FFE), D ** -0.5, 0.125, ((0, 64), (2, 2)))
    expert_down = noise(arg_keys[16], (EXPERTS, FFE, D), FFE ** -0.5, 0.25, ((0, 64), (2, 2)))
    dense_gate = noise(arg_keys[17], (D, FFS), D ** -0.5, 0.125, ((1, 2),))
    dense_up = noise(arg_keys[18], (D, FFS), D ** -0.5, 0.125, ((1, 2),))
    dense_down = noise(arg_keys[19], (FFS, D), FFS ** -0.5, 0.25, ((1, 2),))
    dense_scale = jnp.clip(1.0 + 0.18 * jax.random.normal(arg_keys[20], (D,), jnp.float32), 0.1, 1.9)
    return dict(stream=stream, conv_state=conv_state, recur_state=recur_state, mix_gain=mix_gain, branch_weight=branch_weight, gate_weight=gate_weight, conv_taps=conv_taps, recur_map=recur_map, input_map=input_map, decay_logit=decay_logit, out_weight=out_weight, moe_gain=moe_gain, route_ids=route_ids, route_weights=route_weights, expert_gate=expert_gate, expert_up=expert_up, expert_down=expert_down, dense_gate=dense_gate, dense_up=dense_up, dense_down=dense_down, dense_scale=dense_scale)


def layer_normed(values, gain_vec):
    widened = values.astype(jnp.float32)
    row_mean = lax.optimization_barrier(jnp.mean(widened, axis=-1, keepdims=True))
    row_var = lax.optimization_barrier(jnp.mean(widened * widened, axis=-1, keepdims=True)) - row_mean * row_mean
    return ((widened - row_mean) * lax.rsqrt(row_var + 1e-05) * gain_vec).astype(jnp.bfloat16)

def gated_rows(inputs, w_gate, w_up, w_down):
    gate_sum = jnp.dot(inputs, w_gate, preferred_element_type=jnp.float32)
    up_sum = jnp.dot(inputs, w_up, preferred_element_type=jnp.float32)
    hidden = (jax.nn.silu(gate_sum) * up_sum).astype(jnp.bfloat16)
    return jnp.dot(hidden, w_down, preferred_element_type=jnp.float32).astype(jnp.bfloat16)

def reference(stream, conv_state, recur_state, mix_gain, branch_weight, gate_weight, conv_taps, recur_map, input_map, decay_logit, out_weight, moe_gain, route_ids, route_weights, expert_gate, expert_up, expert_down, dense_gate, dense_up, dense_down, dense_scale):
    normed = layer_normed(stream, mix_gain)
    branch_in = jnp.dot(normed, branch_weight, preferred_element_type=jnp.float32).astype(jnp.bfloat16)
    gate_pre = jnp.dot(normed, gate_weight, preferred_element_type=jnp.float32).astype(jnp.bfloat16)
    conv_sum = branch_in.astype(jnp.float32) * conv_taps[3]
    for offset in range(3):
        conv_sum = conv_sum + conv_state[:, offset].astype(jnp.float32) * conv_taps[offset]
    conv_out = conv_sum.astype(jnp.bfloat16)
    new_conv = jnp.concatenate([conv_state[:, 1:], branch_in[:, None]], axis=1)
    grouped = conv_out.astype(jnp.float32).reshape(BATCH, LBLK, BLK)
    recur_gate = jax.nn.sigmoid(jnp.einsum('nbc,bcd->nbd', grouped, recur_map.astype(jnp.float32))).reshape(BATCH, W)
    input_gate = jax.nn.sigmoid(jnp.einsum('nbc,bcd->nbd', grouped, input_map.astype(jnp.float32))).reshape(BATCH, W)
    log_decay = -8.0 * recur_gate * jax.nn.softplus(-decay_logit)
    driven = jnp.sqrt(-jnp.expm1(2.0 * log_decay)) * (input_gate * conv_out.astype(jnp.float32))
    new_state = jnp.exp(log_decay) * recur_state + driven
    mixer_in = (jax.nn.gelu(gate_pre.astype(jnp.float32)) * new_state).astype(jnp.bfloat16)
    mixer_out = jnp.dot(mixer_in, out_weight, preferred_element_type=jnp.float32).astype(jnp.bfloat16)
    resid = (stream.astype(jnp.float32) + mixer_out.astype(jnp.float32)).astype(jnp.bfloat16)
    normed_two = layer_normed(resid, moe_gain)
    flat_ids = route_ids.reshape(N_EP, SEQ_DEV * TOP)
    one_hot = (flat_ids[:, :, None] == jnp.arange(EXPERTS, dtype=jnp.int32)[None, None, :]).astype(jnp.int32)
    slot_rank = lax.optimization_barrier(jnp.sum(one_hot * (jnp.cumsum(one_hot, axis=1) - 1), axis=2))
    block_ids = jnp.arange(N_EP, dtype=jnp.int32)[:, None]
    column = (block_ids * CAP + slot_rank).reshape(-1).astype(jnp.int32)
    token_ids = (jnp.arange(BATCH * TOP, dtype=jnp.int32) // TOP).astype(jnp.int32)
    row_token = jnp.full((EXPERTS, N_EP * CAP), BATCH, jnp.int32).at[route_ids.reshape(-1), column].set(token_ids)
    padded = jnp.concatenate([normed_two, jnp.zeros((1, D), jnp.bfloat16)], axis=0)

    def one_expert(packed):
        rows_taken, w_gate, w_up, w_down = packed
        return gated_rows(padded[rows_taken], w_gate, w_up, w_down)
    outputs = lax.map(one_expert, (row_token, expert_gate, expert_up, expert_down))
    picked = outputs[route_ids.reshape(-1), column].reshape(BATCH, TOP, D)
    routed = lax.optimization_barrier(jnp.sum(picked.astype(jnp.float32) * route_weights[:, :, None], axis=1))
    dense_out = gated_rows(normed_two, dense_gate, dense_up, dense_down)
    result = (resid.astype(jnp.float32) + routed + dense_scale * dense_out.astype(jnp.float32)).astype(jnp.bfloat16)
    return (result, new_state, new_conv)
```

```python
import functools

import jax
import jax.numpy as jnp
from jax import lax
from jax.experimental import pallas as pl
from jax.experimental.pallas import tpu as pltpu
from jax.sharding import PartitionSpec as P

BF = jnp.bfloat16
F32 = jnp.float32
SWAP = [(0, 1), (1, 0)]
VMEM_LIMIT = 56 * 1024 * 1024


def swapped(x):
    return lax.ppermute(x, "tp", SWAP)


def in_order(core, own, other):
    return jnp.where(
        core == 0,
        jnp.concatenate([own, other], axis=1),
        jnp.concatenate([other, own], axis=1),
    )


def route_tables(ids, core, slots):
    rows = ids.shape[0]
    experts = rows
    lane = lax.broadcasted_iota(jnp.int32, (rows, experts), 1)
    hits = [(ids[:, k : k + 1] == lane) for k in range(ids.shape[1])]
    chosen = functools.reduce(jnp.logical_or, hits)
    chosen_f = jnp.where(chosen, 1.0, 0.0).astype(F32)
    earlier = (
        lax.broadcasted_iota(jnp.int32, (rows, rows), 0)
        > lax.broadcasted_iota(jnp.int32, (rows, rows), 1)
    )
    rank = jnp.dot(
        jnp.where(earlier, 1.0, 0.0).astype(BF),
        chosen_f.astype(BF),
        preferred_element_type=F32,
    )
    place = jnp.where(chosen, rank - (slots * core).astype(F32), -1.0)
    return hits, place


def spread(experts, width):
    lane = lax.broadcasted_iota(jnp.int32, (experts, experts * width), 1)
    sub = lax.broadcasted_iota(jnp.int32, (experts, experts * width), 0)
    return jnp.where(lane // width == sub, 1.0, 0.0).astype(BF)


LANES = 128


def put_pieces(piece_ref, values, start):
    count = values.shape[0]
    for n in range(values.shape[1] // LANES):
        c, part = divmod(start + n, 2)
        piece_ref[part, pl.ds(c, count, stride=8), :] = values[:, n * LANES : (n + 1) * LANES]


def read_pieces(piece_ref):
    return jnp.concatenate([piece_ref[0].astype(BF), piece_ref[1].astype(BF)], axis=1)


def take_pieces(piece_ref, block_ref, features, rows_ref, start):
    count = block_ref.shape[0] // 8
    piece_ref[0] = block_ref[:, features : features + LANES].astype(F32)
    piece_ref[1] = block_ref[:, features + LANES :].astype(F32)
    for n in range(features // LANES):
        c, part = divmod(n, 2)
        rows_ref[start : start + count, n * LANES : (n + 1) * LANES] = piece_ref[
            part, pl.ds(c, count, stride=8), :
        ].astype(BF)


def pack_body(core_ref, own_ref, other_ref, gain_ref, ids_ref, out_ref, norm_ref, piece_ref):
    core = core_ref[0]
    half = own_ref.shape[1]
    features = 2 * half
    own = own_ref[...].astype(F32)
    other = other_ref[...].astype(F32)
    mean = (jnp.sum(own, 1, keepdims=True) + jnp.sum(other, 1, keepdims=True)) / features
    square = (
        jnp.sum(own * own, 1, keepdims=True) + jnp.sum(other * other, 1, keepdims=True)
    ) / features
    scale = lax.rsqrt(square - mean * mean + 1e-05)
    gain_own = gain_ref[pl.ds(core, 1), :]
    gain_other = gain_ref[pl.ds(1 - core, 1), :]
    norm_ref[:, :half] = ((own - mean) * scale * gain_own).astype(BF)
    norm_ref[:, half:] = ((other - mean) * scale * gain_other).astype(BF)
    rows = norm_ref[...]
    experts = ids_ref.shape[0]
    slots = 9
    _, place = route_tables(ids_ref[...], core, slots)
    wide = jnp.dot(place.astype(BF), spread(experts, 8), preferred_element_type=F32)
    lane = lax.broadcasted_iota(jnp.int32, wide.shape, 1) % 8
    table = jnp.where(wide == lane.astype(F32), 1.0, 0.0)
    table = jnp.transpose(table).astype(BF)
    out_ref[:, :features] = jnp.dot(table, rows, preferred_element_type=F32).astype(BF)
    last = jnp.transpose(jnp.where(place == 8.0, 1.0, 0.0)).astype(BF)
    ninth = jnp.dot(last, rows, preferred_element_type=F32)
    put_pieces(piece_ref, ninth, 0)
    out_ref[:, features:] = read_pieces(piece_ref)


def expert_body(
    core_ref,
    in_ref,
    gate_ref,
    gate2_ref,
    up_ref,
    up2_ref,
    down_ref,
    down2_ref,
    out_ref,
    piece_ref,
    rows_ref,
):
    core = core_ref[0]
    count = in_ref.shape[0]
    features = gate_ref.shape[0]
    half = features // 2
    units = gate_ref.shape[1]
    rows_ref[:count, :] = in_ref[:, :features]
    take_pieces(piece_ref, in_ref, features, rows_ref, count)
    first = pl.multiple_of(core * half, half)
    second = pl.multiple_of((1 - core) * half, half)

    def product(weight):
        return jnp.dot(
            rows_ref[:, :half], weight[pl.ds(first, half), :], preferred_element_type=F32
        ) + jnp.dot(rows_ref[:, half:], weight[pl.ds(second, half), :], preferred_element_type=F32)

    def hidden(gate, up):
        return (jax.nn.silu(product(gate)) * product(up)).astype(BF)

    hid_own = hidden(gate_ref, up_ref)
    hid_other = hidden(gate2_ref, up2_ref)
    unit_own = pl.multiple_of(core * units, units)
    unit_other = pl.multiple_of((1 - core) * units, units)
    for part, down in enumerate((down_ref, down2_ref)):
        served = jnp.dot(
            hid_own, down[pl.ds(unit_own, units), :], preferred_element_type=F32
        ) + jnp.dot(hid_other, down[pl.ds(unit_other, units), :], preferred_element_type=F32)
        out_ref[:, part * half : (part + 1) * half] = served[:count].astype(BF)
        put_pieces(piece_ref, served[count:], part * (half // LANES))
    out_ref[:, features:] = read_pieces(piece_ref)


def combine_body(core_ref, in_ref, ids_ref, weights_ref, own_ref, other_ref, piece_ref, last_ref):
    core = core_ref[0]
    experts = ids_ref.shape[0]
    rows = ids_ref.shape[0]
    features = 2 * own_ref.shape[1]
    half = features // 2
    hits, place = route_tables(ids_ref[...], core, 9)
    weight = functools.reduce(
        jnp.add,
        [jnp.where(hit, weights_ref[:, k : k + 1], 0.0) for k, hit in enumerate(hits)],
    )
    high = weight.astype(BF).astype(F32)
    low = (weight - high).astype(BF).astype(F32)
    expand = spread(experts, 8)
    wide = jnp.dot(place.astype(BF), expand, preferred_element_type=F32)
    lane = lax.broadcasted_iota(jnp.int32, wide.shape, 1) % 8
    match = wide == lane.astype(F32)
    tables = []
    lasts = []
    for part in (high, low):
        spread_part = jnp.dot(part.astype(BF), expand, preferred_element_type=F32)
        tables.append(jnp.where(match, spread_part, 0.0).astype(BF))
        lasts.append(jnp.where(place == 8.0, part, 0.0).astype(BF))
    table = jnp.concatenate(tables, axis=0)
    last = jnp.concatenate(lasts, axis=0)
    take_pieces(piece_ref, in_ref, features, last_ref, 0)
    total = jnp.dot(table, in_ref[:, :features], preferred_element_type=F32) + jnp.dot(
        last, last_ref[...], preferred_element_type=F32
    )
    total = total[:rows] + total[rows:]
    own_ref[...] = total[:, :half]
    other_ref[...] = total[:, half:]


def vmem(count):
    return [pl.BlockSpec(memory_space=pltpu.VMEM)] * count


def smem():
    return [pl.BlockSpec(memory_space=pltpu.SMEM)]


def per_device(
    stream,
    conv_state,
    recur_state,
    mix_gain,
    branch_weight,
    gate_weight,
    conv_taps,
    recur_map,
    input_map,
    decay_logit,
    out_weight,
    moe_gain,
    route_ids,
    route_weights,
    expert_gate,
    expert_up,
    expert_down,
    dense_gate,
    dense_up,
    dense_down,
    dense_scale,
):
    core = lax.axis_index("tp")
    core_arr = core.astype(jnp.int32).reshape(1)
    seq_count, half = stream.shape
    features = 2 * half
    experts = lax.axis_size("ep")
    own_gate, own_up, own_down = expert_gate[0], expert_up[0], expert_down[0]
    stream_other = swapped(stream)
    other_gate, other_up, other_down = swapped(own_gate), swapped(own_up), swapped(own_down)

    whole = in_order(core, stream, stream_other).astype(F32)
    mean = jnp.mean(whole, axis=1, keepdims=True)
    var = jnp.mean(whole * whole, axis=1, keepdims=True) - mean * mean
    normed = ((whole - mean) * lax.rsqrt(var + 1e-05) * mix_gain).astype(BF)
    branch_in = jnp.dot(normed, branch_weight, preferred_element_type=F32).astype(BF)
    gate_pre = jnp.dot(normed, gate_weight, preferred_element_type=F32).astype(BF)
    conv_sum = branch_in.astype(F32) * conv_taps[3]
    for offset in range(3):
        conv_sum = conv_sum + conv_state[:, offset].astype(F32) * conv_taps[offset]
    conv_out = conv_sum.astype(BF)
    new_conv = jnp.concatenate([conv_state[:, 1:], branch_in[:, None]], axis=1)
    block_count, block_width = recur_map.shape[0], recur_map.shape[1]
    grouped = conv_out.reshape(seq_count, block_count, block_width)
    recur_gate = jax.nn.sigmoid(
        jnp.einsum("nbc,bcd->nbd", grouped, recur_map, preferred_element_type=F32)
    ).reshape(seq_count, -1)
    input_gate = jax.nn.sigmoid(
        jnp.einsum("nbc,bcd->nbd", grouped, input_map, preferred_element_type=F32)
    ).reshape(seq_count, -1)
    log_decay = -8.0 * recur_gate * jax.nn.softplus(-decay_logit)
    driven = jnp.sqrt(-jnp.expm1(2.0 * log_decay)) * (input_gate * conv_out.astype(F32))
    new_state = jnp.exp(log_decay) * recur_state + driven
    mixer_in = (jax.nn.gelu(gate_pre.astype(F32)) * new_state).astype(BF)
    mixer_whole = in_order(core, mixer_in, swapped(mixer_in))
    mixer_out = jnp.dot(mixer_whole, out_weight, preferred_element_type=F32).astype(BF)
    resid = (stream.astype(F32) + mixer_out.astype(F32)).astype(BF)
    resid_other = swapped(resid)

    block = features + features // 8
    payload, normed_two = pl.pallas_call(
        pack_body,
        name="pack",
        out_shape=(
            jax.ShapeDtypeStruct((experts * 8, block), BF),
            jax.ShapeDtypeStruct((seq_count, features), BF),
        ),
        in_specs=smem() + vmem(4),
        out_specs=tuple(vmem(2)),
        scratch_shapes=[pltpu.VMEM((2, experts * 8, LANES), F32)],
        compiler_params=pltpu.CompilerParams(vmem_limit_bytes=VMEM_LIMIT),
    )(core_arr, resid, resid_other, moe_gain.reshape(2, half), route_ids)

    incoming = lax.all_to_all(
        payload.reshape(experts, 8, block), "ep", split_axis=0, concat_axis=0, tiled=True
    ).reshape(experts * 8, block)

    own_two, other_two = normed_two[:, :half], normed_two[:, half:]
    whole_two = in_order(core, own_two, other_two)
    dense_hidden = (
        jax.nn.silu(jnp.dot(whole_two, dense_gate, preferred_element_type=F32))
        * jnp.dot(whole_two, dense_up, preferred_element_type=F32)
    ).astype(BF)
    dense_whole = in_order(core, dense_hidden, swapped(dense_hidden))
    dense_out = jnp.dot(dense_whole, dense_down, preferred_element_type=F32).astype(BF)
    base = resid.astype(F32) + dense_scale * dense_out.astype(F32)

    served = pl.pallas_call(
        expert_body,
        name="experts",
        out_shape=jax.ShapeDtypeStruct((experts * 8, block), BF),
        in_specs=smem() + vmem(7),
        out_specs=vmem(1)[0],
        scratch_shapes=[
            pltpu.VMEM((2, experts * 8, LANES), F32),
            pltpu.VMEM((experts * 9, features), BF),
        ],
        compiler_params=pltpu.CompilerParams(vmem_limit_bytes=VMEM_LIMIT),
    )(
        core_arr,
        incoming,
        own_gate,
        other_gate,
        own_up,
        other_up,
        own_down,
        other_down,
    )

    returned = lax.all_to_all(
        served.reshape(experts, 8, block), "ep", split_axis=0, concat_axis=0, tiled=True
    ).reshape(experts * 8, block)

    sum_own, sum_other = pl.pallas_call(
        combine_body,
        name="combine",
        out_shape=(
            jax.ShapeDtypeStruct((seq_count, half), F32),
            jax.ShapeDtypeStruct((seq_count, half), F32),
        ),
        in_specs=smem() + vmem(3),
        out_specs=tuple(vmem(2)),
        scratch_shapes=[
            pltpu.VMEM((2, experts * 8, LANES), F32),
            pltpu.VMEM((experts, features), BF),
        ],
        compiler_params=pltpu.CompilerParams(vmem_limit_bytes=VMEM_LIMIT),
    )(core_arr, returned, route_ids, route_weights)
    result = (base + (sum_own + swapped(sum_other))).astype(BF)
    return (result, new_state, new_conv)


def solution(mesh):
    in_specs = (
        P("ep", "tp"),
        P("ep", None, "tp"),
        P("ep", "tp"),
        P(),
        P(None, "tp"),
        P(None, "tp"),
        P(None, "tp"),
        P("tp", None, None),
        P("tp", None, None),
        P("tp"),
        P(None, "tp"),
        P(),
        P("ep", None),
        P("ep", None),
        P("ep", None, "tp"),
        P("ep", None, "tp"),
        P("ep", None, "tp"),
        P(None, "tp"),
        P(None, "tp"),
        P(None, "tp"),
        P("tp"),
    )
    out_specs = (P("ep", "tp"), P("ep", "tp"), P("ep", None, "tp"))
    return jax.shard_map(
        per_device, mesh=mesh, in_specs=in_specs, out_specs=out_specs, check_vma=False
    )
```

```python
import functools

import jax
import jax.numpy as jnp
from jax import lax
from jax.experimental import pallas as pl
from jax.experimental.pallas import tpu as pltpu
from jax.sharding import PartitionSpec as P


BF = jnp.bfloat16
F32 = jnp.float32
SWAP = [(0, 1), (1, 0)]
MIB = 1024 * 1024
LANES = 128
SLOTS = 9
MAIN = 8
CHUNKS = 4


def swapped(x):
    return lax.ppermute(x, "tp", SWAP)


def in_order(core, own, other):
    return jnp.where(
        core == 0,
        jnp.concatenate([own, other], axis=1),
        jnp.concatenate([other, own], axis=1),
    )


def places(ids, core):
    experts = rows = ids.shape[1]
    expert = lax.broadcasted_iota(jnp.int32, (experts, rows), 0)
    hits = [ids[k : k + 1, :] == expert for k in range(ids.shape[0])]
    chosen = functools.reduce(jnp.logical_or, hits)
    earlier = lax.broadcasted_iota(jnp.int32, (rows, rows), 0) < lax.broadcasted_iota(
        jnp.int32, (rows, rows), 1
    )
    rank = jnp.dot(
        jnp.where(chosen, 1.0, 0.0).astype(BF),
        jnp.where(earlier, 1.0, 0.0).astype(BF),
        preferred_element_type=F32,
    )
    return hits, jnp.where(chosen, rank - (SLOTS * core).astype(F32), -1.0)


def each_slot(values):
    experts = values.shape[0]
    shape = (experts * MAIN, experts)
    row = lax.broadcasted_iota(jnp.int32, shape, 0) // MAIN
    spread = jnp.where(row == lax.broadcasted_iota(jnp.int32, shape, 1), 1.0, 0.0).astype(BF)
    return jnp.dot(spread, values.astype(BF), preferred_element_type=F32)


def slot_number(shape):
    return (lax.broadcasted_iota(jnp.int32, shape, 0) % MAIN).astype(F32)


def put_pieces(piece_ref, values, start, base):
    count = values.shape[0]
    for n in range(values.shape[1] // LANES):
        c, part = divmod(start + n, 2)
        piece_ref[part, pl.ds(base + c, count, stride=MAIN), :] = values[
            :, n * LANES : (n + 1) * LANES
        ]


def take_pieces(piece_ref, block_ref, features, rows_ref, start):
    count = block_ref.shape[0] // MAIN
    piece_ref[0] = block_ref[:, features : features + LANES].astype(F32)
    piece_ref[1] = block_ref[:, features + LANES :].astype(F32)
    for n in range(features // LANES):
        c, part = divmod(n, 2)
        rows_ref[start : start + count, n * LANES : (n + 1) * LANES] = piece_ref[
            part, pl.ds(c, count, stride=MAIN), :
        ].astype(BF)


def pack_body(
    core_ref,
    own_ref,
    other_ref,
    gain_ref,
    ids_ref,
    out_ref,
    norm_out_ref,
    norm_ref,
    block_ref,
    piece_ref,
    sems,
):
    core = core_ref[0]
    half = own_ref.shape[1]
    features = 2 * half
    own = own_ref[...].astype(F32)
    other = other_ref[...].astype(F32)
    mean = (jnp.sum(own, 1, keepdims=True) + jnp.sum(other, 1, keepdims=True)) / features
    square = (
        jnp.sum(own * own, 1, keepdims=True) + jnp.sum(other * other, 1, keepdims=True)
    ) / features
    scale = lax.rsqrt(square - mean * mean + 1e-05)
    low, high = gain_ref[:, :half], gain_ref[:, half:]
    gain_own = jnp.where(core == 0, low, high)
    gain_other = jnp.where(core == 0, high, low)
    norm_ref[:, :half] = ((own - mean) * scale * gain_own).astype(BF)
    norm_ref[:, half:] = ((other - mean) * scale * gain_other).astype(BF)
    norm_copy = pltpu.make_async_copy(norm_ref, norm_out_ref, sems.at[CHUNKS])
    norm_copy.start()
    rows = norm_ref[...]
    experts = ids_ref.shape[1]
    _, place = places(ids_ref[...], core)
    wide = each_slot(place)
    table = jnp.where(wide == slot_number(wide.shape), 1.0, 0.0).astype(BF)
    last = jnp.where(place == float(MAIN), 1.0, 0.0).astype(BF)
    ninth = jnp.dot(last, rows, preferred_element_type=F32)
    put_pieces(piece_ref, ninth, 0, 0)
    count = experts * MAIN
    step = count // CHUNKS
    copies = [norm_copy]
    for n in range(CHUNKS):
        span = slice(n * step, (n + 1) * step)
        block_ref[span, :features] = jnp.dot(
            table[span], rows, preferred_element_type=F32
        ).astype(BF)
        block_ref[span, features : features + LANES] = piece_ref[0, span].astype(BF)
        block_ref[span, features + LANES :] = piece_ref[1, span].astype(BF)
        copy = pltpu.make_async_copy(block_ref.at[span], out_ref.at[span], sems.at[n])
        copy.start()
        copies.append(copy)
    for copy in copies:
        copy.wait()


def table_body(core_ref, ids_ref, weights_ref, table_ref, last_ref):
    rows = ids_ref.shape[1]
    hits, place = places(ids_ref[...], core_ref[0])
    weight = functools.reduce(
        jnp.add,
        [jnp.where(hit, weights_ref[k : k + 1, :], 0.0) for k, hit in enumerate(hits)],
    )
    high = weight.astype(BF).astype(F32)
    low = (weight - high).astype(BF).astype(F32)
    wide = each_slot(place)
    match = wide == slot_number(wide.shape)
    for n, part in enumerate((high, low)):
        span = slice(n * rows, (n + 1) * rows)
        table_ref[span, :] = jnp.transpose(jnp.where(match, each_slot(part), 0.0)).astype(BF)
        last_ref[span, :] = jnp.transpose(jnp.where(place == float(MAIN), part, 0.0)).astype(BF)


def expert_body(
    core_ref,
    in_ref,
    gate_ref,
    gate2_ref,
    up_ref,
    up2_ref,
    down_ref,
    down2_ref,
    out_ref,
    gates_ref,
    ups_ref,
    downs_ref,
    block_ref,
    piece_ref,
    take_ref,
    rows_ref,
    sems,
    out_sems,
):
    core = core_ref[0]
    features, units = gate_ref.shape
    half = features // 2
    starts = (pl.multiple_of(core * half, half), pl.multiple_of((1 - core) * half, half))
    unit_starts = (
        pl.multiple_of(core * units, units),
        pl.multiple_of((1 - core) * units, units),
    )
    loads = []
    for whole, parts, size, width, offsets in (
        (gates_ref, (gate_ref, gate2_ref), half, units, starts),
        (ups_ref, (up_ref, up2_ref), half, units, starts),
        (downs_ref, (down_ref, down2_ref), units, half, unit_starts),
    ):
        group = []
        for column, part in enumerate(parts):
            for row, start in enumerate(offsets):
                copy = pltpu.make_async_copy(
                    part.at[pl.ds(start, size), :],
                    whole.at[pl.ds(row * size, size), pl.ds(column * width, width)],
                    sems.at[4 * len(loads) + len(group)],
                )
                copy.start()
                group.append(copy)
        loads.append(group)
    count = in_ref.shape[0]
    step = count // CHUNKS
    take_pieces(take_ref, in_ref, features, rows_ref, 0)
    main, last = in_ref[:, :features], rows_ref[...]

    def product(weight):
        return jnp.concatenate(
            [
                jnp.dot(main, weight, preferred_element_type=F32),
                jnp.dot(last, weight, preferred_element_type=F32),
            ],
            axis=0,
        )

    for copy in loads[0]:
        copy.wait()
    gate = product(gates_ref[...])
    for copy in loads[1]:
        copy.wait()
    hidden = (jax.nn.silu(gate) * product(ups_ref[...])).astype(BF)
    for copy in loads[2]:
        copy.wait()
    served = jnp.dot(hidden[count:], downs_ref[...], preferred_element_type=F32)
    put_pieces(piece_ref, served, 0, 0)
    copies = []
    for n in range(CHUNKS):
        span = slice(n * step, (n + 1) * step)
        block_ref[span, :features] = jnp.dot(
            hidden[span], downs_ref[...], preferred_element_type=F32
        ).astype(BF)
        block_ref[span, features : features + LANES] = piece_ref[0, span].astype(BF)
        block_ref[span, features + LANES :] = piece_ref[1, span].astype(BF)
        copy = pltpu.make_async_copy(block_ref.at[span], out_ref.at[span], out_sems.at[n])
        copy.start()
        copies.append(copy)
    for copy in copies:
        copy.wait()


def combine_body(in_ref, table_ref, lasts_ref, own_ref, other_ref, piece_ref, last_ref):
    rows, half = own_ref.shape
    features = 2 * half
    take_pieces(piece_ref, in_ref, features, last_ref, 0)
    total = jnp.dot(
        table_ref[...], in_ref[:, :features], preferred_element_type=F32
    ) + jnp.dot(lasts_ref[...], last_ref[...], preferred_element_type=F32)
    total = total[:rows] + total[rows:]
    own_ref[...] = total[:, :half]
    other_ref[...] = total[:, half:]


def vmem(count):
    return [pl.BlockSpec(memory_space=pltpu.VMEM)] * count


def hbm(count):
    return [pl.BlockSpec(memory_space=pltpu.HBM)] * count


def smem():
    return [pl.BlockSpec(memory_space=pltpu.SMEM)]


def per_device(
    stream,
    conv_state,
    recur_state,
    mix_gain,
    branch_weight,
    gate_weight,
    conv_taps,
    recur_map,
    input_map,
    decay_logit,
    out_weight,
    moe_gain,
    route_ids,
    route_weights,
    expert_gate,
    expert_up,
    expert_down,
    dense_gate,
    dense_up,
    dense_down,
    dense_scale,
):
    core = lax.axis_index("tp")
    core_arr = core.astype(jnp.int32).reshape(1)
    seq_count, half = stream.shape
    features = 2 * half
    experts = lax.axis_size("ep")
    own_gate, own_up, own_down = expert_gate[0], expert_up[0], expert_down[0]
    stream_other = swapped(stream)

    whole = in_order(core, stream, stream_other).astype(F32)
    mean = jnp.mean(whole, axis=1, keepdims=True)
    var = jnp.mean(whole * whole, axis=1, keepdims=True) - mean * mean
    normed = ((whole - mean) * lax.rsqrt(var + 1e-05) * mix_gain).astype(BF)
    branch_in = jnp.dot(normed, branch_weight, preferred_element_type=F32).astype(BF)
    gate_pre = jnp.dot(normed, gate_weight, preferred_element_type=F32).astype(BF)
    conv_sum = branch_in.astype(F32) * conv_taps[3]
    for offset in range(3):
        conv_sum = conv_sum + conv_state[:, offset].astype(F32) * conv_taps[offset]
    conv_out = conv_sum.astype(BF)
    new_conv = jnp.concatenate([conv_state[:, 1:], branch_in[:, None]], axis=1)
    block_count, block_width = recur_map.shape[0], recur_map.shape[1]
    grouped = conv_out.reshape(seq_count, block_count, block_width)
    recur_gate = jax.nn.sigmoid(
        jnp.einsum("nbc,bcd->nbd", grouped, recur_map, preferred_element_type=F32)
    ).reshape(seq_count, -1)
    input_gate = jax.nn.sigmoid(
        jnp.einsum("nbc,bcd->nbd", grouped, input_map, preferred_element_type=F32)
    ).reshape(seq_count, -1)
    log_decay = -8.0 * recur_gate * jax.nn.softplus(-decay_logit)
    driven = jnp.sqrt(-jnp.expm1(2.0 * log_decay)) * (input_gate * conv_out.astype(F32))
    new_state = jnp.exp(log_decay) * recur_state + driven
    mixer_in = (jax.nn.gelu(gate_pre.astype(F32)) * new_state).astype(BF)
    mixer_whole = in_order(core, mixer_in, swapped(mixer_in))
    mixer_out = jnp.dot(mixer_whole, out_weight, preferred_element_type=F32).astype(BF)
    resid = (stream.astype(F32) + mixer_out.astype(F32)).astype(BF)
    resid_other = swapped(resid)

    block = features + features // MAIN
    count = experts * MAIN
    pieces = pltpu.VMEM((2, count, LANES), F32)
    ids_t, weights_t = route_ids.T, route_weights.T
    payload, normed_two = pl.pallas_call(
        pack_body,
        name="pack",
        out_shape=(pltpu.HBM((count, block), BF), pltpu.HBM((seq_count, features), BF)),
        in_specs=smem() + vmem(4),
        out_specs=tuple(hbm(2)),
        scratch_shapes=[
            pltpu.VMEM((seq_count, features), BF),
            pltpu.VMEM((count, block), BF),
            pieces,
            pltpu.SemaphoreType.DMA((CHUNKS + 1,)),
        ],
        compiler_params=pltpu.CompilerParams(vmem_limit_bytes=14 * MIB),
    )(core_arr, resid, resid_other, moe_gain.reshape(1, features), ids_t)

    own_gate, own_up, own_down, payload = lax.optimization_barrier(
        (own_gate, own_up, own_down, payload)
    )
    other_gate, other_up, other_down = swapped(own_gate), swapped(own_up), swapped(own_down)
    incoming = lax.all_to_all(
        payload.reshape(experts, MAIN, block), "ep", split_axis=0, concat_axis=0, tiled=True
    )
    incoming = incoming.reshape(count, block)
    units = own_gate.shape[1]
    table, last = pl.pallas_call(
        table_body,
        name="table",
        out_shape=(
            jax.ShapeDtypeStruct((2 * seq_count, count), BF),
            jax.ShapeDtypeStruct((2 * seq_count, experts), BF),
        ),
        in_specs=smem() + vmem(2),
        out_specs=tuple(vmem(2)),
        compiler_params=pltpu.CompilerParams(vmem_limit_bytes=8 * MIB),
    )(core_arr, ids_t, weights_t)

    own_two, other_two = normed_two[:, :half], normed_two[:, half:]
    whole_two = in_order(core, own_two, other_two)
    dense_hidden = (
        jax.nn.silu(jnp.dot(whole_two, dense_gate, preferred_element_type=F32))
        * jnp.dot(whole_two, dense_up, preferred_element_type=F32)
    ).astype(BF)
    dense_whole = in_order(core, dense_hidden, swapped(dense_hidden))
    dense_out = jnp.dot(dense_whole, dense_down, preferred_element_type=F32).astype(BF)
    base = resid.astype(F32) + dense_scale * dense_out.astype(F32)

    incoming, base, new_conv, new_state, table, last = lax.optimization_barrier(
        (incoming, base, new_conv, new_state, table, last)
    )
    served = pl.pallas_call(
        expert_body,
        name="experts",
        out_shape=pltpu.HBM((count, block), BF),
        in_specs=smem() + vmem(1) + hbm(6),
        out_specs=hbm(1)[0],
        scratch_shapes=[
            pltpu.VMEM((features, 2 * units), BF),
            pltpu.VMEM((features, 2 * units), BF),
            pltpu.VMEM((2 * units, features), BF),
            pltpu.VMEM((count, block), BF),
            pieces,
            pieces,
            pltpu.VMEM((experts, features), BF),
            pltpu.SemaphoreType.DMA((12,)),
            pltpu.SemaphoreType.DMA((CHUNKS,)),
        ],
        compiler_params=pltpu.CompilerParams(vmem_limit_bytes=28 * MIB),
    )(
        core_arr,
        incoming,
        *(
            pltpu.with_memory_space_constraint(weight, pltpu.HBM)
            for weight in (own_gate, other_gate, own_up, other_up, own_down, other_down)
        ),
    )

    returned = lax.all_to_all(
        served.reshape(experts, MAIN, block), "ep", split_axis=0, concat_axis=0, tiled=True
    )
    returned = returned.reshape(count, block)
    sum_own, sum_other = pl.pallas_call(
        combine_body,
        name="combine",
        out_shape=(
            jax.ShapeDtypeStruct((seq_count, half), F32),
            jax.ShapeDtypeStruct((seq_count, half), F32),
        ),
        in_specs=vmem(3),
        out_specs=tuple(vmem(2)),
        scratch_shapes=[pieces, pltpu.VMEM((experts, features), BF)],
        compiler_params=pltpu.CompilerParams(vmem_limit_bytes=14 * MIB),
    )(returned, table, last)
    result = (base + (sum_own + swapped(sum_other))).astype(BF)
    return (result, new_state, new_conv)


def solution(mesh):
    in_specs = (
        P("ep", "tp"),
        P("ep", None, "tp"),
        P("ep", "tp"),
        P(),
        P(None, "tp"),
        P(None, "tp"),
        P(None, "tp"),
        P("tp", None, None),
        P("tp", None, None),
        P("tp"),
        P(None, "tp"),
        P(),
        P("ep", None),
        P("ep", None),
        P("ep", None, "tp"),
        P("ep", None, "tp"),
        P("ep", None, "tp"),
        P(None, "tp"),
        P(None, "tp"),
        P(None, "tp"),
        P("tp"),
    )
    out_specs = (P("ep", "tp"), P("ep", "tp"), P("ep", None, "tp"))
    return jax.shard_map(
        per_device, mesh=mesh, in_specs=in_specs, out_specs=out_specs, check_vma=False
    )
```

```python
import functools

import jax
import jax.numpy as jnp
from jax import lax
from jax.experimental import pallas as pl
from jax.experimental.pallas import tpu as pltpu
from jax.sharding import PartitionSpec as P


BF = jnp.bfloat16
F32 = jnp.float32
SWAP = [(0, 1), (1, 0)]
MIB = 1024 * 1024
LANES = 128
SLOTS = 9
MAIN = 8


def swapped(x):
    return lax.ppermute(x, "tp", SWAP)


def in_order(core, own, other):
    return jnp.where(
        core == 0,
        jnp.concatenate([own, other], axis=1),
        jnp.concatenate([other, own], axis=1),
    )


def places(ids, core):
    experts = rows = ids.shape[1]
    expert = lax.broadcasted_iota(jnp.int32, (experts, rows), 0)
    hits = [ids[k : k + 1, :] == expert for k in range(ids.shape[0])]
    chosen = functools.reduce(jnp.logical_or, hits)
    earlier = lax.broadcasted_iota(jnp.int32, (rows, rows), 0) < lax.broadcasted_iota(
        jnp.int32, (rows, rows), 1
    )
    rank = jnp.dot(
        jnp.where(chosen, 1.0, 0.0).astype(BF),
        jnp.where(earlier, 1.0, 0.0).astype(BF),
        preferred_element_type=F32,
    )
    return hits, jnp.where(chosen, rank - (SLOTS * core).astype(F32), -1.0)


def each_slot(values):
    experts = values.shape[0]
    shape = (experts * MAIN, experts)
    row = lax.broadcasted_iota(jnp.int32, shape, 0) // MAIN
    spread = jnp.where(row == lax.broadcasted_iota(jnp.int32, shape, 1), 1.0, 0.0).astype(BF)
    return jnp.dot(spread, values.astype(BF), preferred_element_type=F32)


def slot_number(shape):
    return (lax.broadcasted_iota(jnp.int32, shape, 0) % MAIN).astype(F32)


def put_pieces(piece_ref, values, start, base):
    count = values.shape[0]
    for n in range(values.shape[1] // LANES):
        c, part = divmod(start + n, 2)
        piece_ref[part, pl.ds(base + c, count, stride=MAIN), :] = values[
            :, n * LANES : (n + 1) * LANES
        ]


def take_pieces(piece_ref, block_ref, features, rows_ref, start):
    count = block_ref.shape[0] // MAIN
    piece_ref[0] = block_ref[:, features : features + LANES].astype(F32)
    piece_ref[1] = block_ref[:, features + LANES :].astype(F32)
    for n in range(features // LANES):
        c, part = divmod(n, 2)
        rows_ref[start : start + count, n * LANES : (n + 1) * LANES] = piece_ref[
            part, pl.ds(c, count, stride=MAIN), :
        ].astype(BF)


def pack_body(
    core_ref,
    own_ref,
    other_ref,
    gain_ref,
    ids_ref,
    out_ref,
    norm_out_ref,
    norm_ref,
    piece_ref,
    sem,
):
    core = core_ref[0]
    half = own_ref.shape[1]
    features = 2 * half
    own = own_ref[...].astype(F32)
    other = other_ref[...].astype(F32)
    mean = (jnp.sum(own, 1, keepdims=True) + jnp.sum(other, 1, keepdims=True)) / features
    square = (
        jnp.sum(own * own, 1, keepdims=True) + jnp.sum(other * other, 1, keepdims=True)
    ) / features
    scale = lax.rsqrt(square - mean * mean + 1e-05)
    low, high = gain_ref[:, :half], gain_ref[:, half:]
    gain_own = jnp.where(core == 0, low, high)
    gain_other = jnp.where(core == 0, high, low)
    norm_ref[:, :half] = ((own - mean) * scale * gain_own).astype(BF)
    norm_ref[:, half:] = ((other - mean) * scale * gain_other).astype(BF)
    norm_copy = pltpu.make_async_copy(norm_ref, norm_out_ref, sem)
    norm_copy.start()
    rows = norm_ref[...]
    _, place = places(ids_ref[...], core)
    wide = each_slot(place)
    table = jnp.where(wide == slot_number(wide.shape), 1.0, 0.0).astype(BF)
    last = jnp.where(place == float(MAIN), 1.0, 0.0).astype(BF)
    out_ref[:, :features] = jnp.dot(table, rows, preferred_element_type=F32).astype(BF)
    put_pieces(piece_ref, jnp.dot(last, rows, preferred_element_type=F32), 0, 0)
    out_ref[:, features : features + LANES] = piece_ref[0].astype(BF)
    out_ref[:, features + LANES :] = piece_ref[1].astype(BF)
    norm_copy.wait()


def start_all(pairs, sems):
    copies = [
        pltpu.make_async_copy(source, target, sems.at[n])
        for n, (source, target) in enumerate(pairs)
    ]
    for copy in copies:
        copy.start()
    return copies


def wait_all(copies):
    for copy in copies:
        copy.wait()


def warm_body(
    weight_hbm,
    state_hbm,
    taps_hbm,
    logit_hbm,
    weight_ref,
    conv_ref,
    decay_ref,
    state_ref,
    taps_ref,
    logit_ref,
    sems,
):
    copies = start_all(
        (
            (state_hbm, state_ref),
            (taps_hbm, taps_ref),
            (logit_hbm, logit_ref),
            (weight_hbm, weight_ref),
        ),
        sems,
    )
    wait_all(copies[:3])
    conv = state_ref[0].astype(F32) * taps_ref[0:1, :]
    for offset in range(1, 3):
        conv = conv + state_ref[offset].astype(F32) * taps_ref[offset : offset + 1, :]
    conv_ref[...] = conv
    decay_ref[...] = -8.0 * jax.nn.softplus(-logit_ref[...])
    wait_all(copies[3:])


def near_body(core_ref, mixed_ref, weight_ref, weight_hbm, part_ref, other_ref, sem):
    half = mixed_ref.shape[1]
    second = pl.ds(pl.multiple_of((1 - core_ref[0]) * half, half), half)
    copy = pltpu.make_async_copy(weight_hbm.at[second, :], other_ref, sem)
    copy.start()
    part_ref[...] = jnp.dot(mixed_ref[...], weight_ref[...], preferred_element_type=F32)
    copy.wait()


def resid_body(part_ref, mixed_ref, weight_ref, stream_ref, out_ref):
    mixer_out = part_ref[...] + jnp.dot(
        mixed_ref[...], weight_ref[...], preferred_element_type=F32
    )
    out_ref[...] = (stream_ref[...].astype(F32) + mixer_out.astype(BF).astype(F32)).astype(BF)


def mixer_body(
    core_ref,
    own_ref,
    other_ref,
    gain_ref,
    branch_ref,
    conv_ref,
    taps_ref,
    decay_ref,
    recur_ref,
    input_ref,
    state_ref,
    gate_hbm,
    out_hbm,
    branch_out_hbm,
    state_out_hbm,
    mixed_ref,
    weight_ref,
    gate_ref,
    branch_out_ref,
    state_out_ref,
    sems,
):
    core = core_ref[0]
    half = own_ref.shape[1]
    features = 2 * half
    first = pl.ds(pl.multiple_of(core * half, half), half)
    second = pl.ds(pl.multiple_of((1 - core) * half, half), half)
    copies = start_all(((gate_hbm, gate_ref), (out_hbm.at[first, :], weight_ref)), sems)
    own = own_ref[...].astype(F32)
    other = other_ref[...].astype(F32)
    mean = (jnp.sum(own, 1, keepdims=True) + jnp.sum(other, 1, keepdims=True)) / features
    square = (
        jnp.sum(own * own, 1, keepdims=True) + jnp.sum(other * other, 1, keepdims=True)
    ) / features
    scale = lax.rsqrt(square - mean * mean + 1e-05)
    low, high = gain_ref[:, :half], gain_ref[:, half:]
    own = ((own - mean) * scale * jnp.where(core == 0, low, high)).astype(BF)
    other = ((other - mean) * scale * jnp.where(core == 0, high, low)).astype(BF)

    def product(weight):
        return (
            jnp.dot(own, weight[first, :], preferred_element_type=F32)
            + jnp.dot(other, weight[second, :], preferred_element_type=F32)
        ).astype(BF)

    branch = product(branch_ref)
    branch_out_ref[...] = branch
    conv = (conv_ref[...] + branch.astype(F32) * taps_ref[3:4, :]).astype(BF)
    width = recur_ref.shape[1]
    recur, drive = (
        jnp.concatenate(
            [
                jnp.dot(
                    conv[:, n * width : (n + 1) * width], maps[n], preferred_element_type=F32
                )
                for n in range(maps.shape[0])
            ],
            axis=1,
        )
        for maps in (recur_ref, input_ref)
    )
    log_decay = jax.nn.sigmoid(recur) * decay_ref[...]
    turn = jnp.tanh(log_decay)
    kept = jnp.sqrt(-2.0 * turn / (1.0 - turn))
    driven = kept * (jax.nn.sigmoid(drive) * conv.astype(F32))
    state = jnp.exp(log_decay) * state_ref[...] + driven
    state_out_ref[...] = state
    branch_copy = pltpu.make_async_copy(branch_out_ref, branch_out_hbm, sems.at[2])
    branch_copy.start()
    state_copy = pltpu.make_async_copy(state_out_ref, state_out_hbm, sems.at[3])
    state_copy.start()
    wait_all(copies[:1])
    mixed_ref[...] = (jax.nn.gelu(product(gate_ref).astype(F32)) * state).astype(BF)
    wait_all([*copies[1:], branch_copy, state_copy])


def table_body(core_ref, ids_ref, weights_ref, table_ref, last_ref):
    rows = ids_ref.shape[1]
    hits, place = places(ids_ref[...], core_ref[0])
    weight = functools.reduce(
        jnp.add,
        [jnp.where(hit, weights_ref[k : k + 1, :], 0.0) for k, hit in enumerate(hits)],
    )
    high = weight.astype(BF).astype(F32)
    low = (weight - high).astype(BF).astype(F32)
    wide = each_slot(place)
    match = wide == slot_number(wide.shape)
    for n, part in enumerate((high, low)):
        span = slice(n * rows, (n + 1) * rows)
        table_ref[span, :] = jnp.transpose(jnp.where(match, each_slot(part), 0.0)).astype(BF)
        last_ref[span, :] = jnp.transpose(jnp.where(place == float(MAIN), part, 0.0)).astype(BF)


def expert_body(
    core_ref,
    in_ref,
    gate_ref,
    gate2_ref,
    up_ref,
    up2_ref,
    down_ref,
    down2_ref,
    out_ref,
    block_ref,
    piece_ref,
    take_ref,
    rows_ref,
    out_sems,
):
    core = core_ref[0]
    features, units = gate_ref.shape
    half = features // 2
    first = pl.ds(pl.multiple_of(core * half, half), half)
    second = pl.ds(pl.multiple_of((1 - core) * half, half), half)
    unit_own = pl.ds(pl.multiple_of(core * units, units), units)
    unit_other = pl.ds(pl.multiple_of((1 - core) * units, units), units)
    count = in_ref.shape[0]
    extra = count // MAIN
    take_pieces(take_ref, in_ref, features, rows_ref, 0)
    rows_ref[extra:, :] = in_ref[:, :features]

    def product(weight):
        return jnp.dot(
            rows_ref[:, :half], weight[first, :], preferred_element_type=F32
        ) + jnp.dot(rows_ref[:, half:], weight[second, :], preferred_element_type=F32)

    def hidden(gate, up):
        return (jax.nn.silu(product(gate)) * product(up)).astype(BF)

    hid_own = hidden(gate_ref, up_ref)
    hid_other = hidden(gate2_ref, up2_ref)
    copies = []
    for part, down in enumerate((down_ref, down2_ref)):
        served = jnp.dot(hid_own, down[unit_own, :], preferred_element_type=F32) + jnp.dot(
            hid_other, down[unit_other, :], preferred_element_type=F32
        )
        put_pieces(piece_ref, served[:extra], part * (half // LANES), 0)
        cols = slice(part * half, (part + 1) * half)
        block_ref[:, cols] = served[extra:].astype(BF)
        if part:
            cols = slice(half, block_ref.shape[1])
            block_ref[:, features : features + LANES] = piece_ref[0].astype(BF)
            block_ref[:, features + LANES :] = piece_ref[1].astype(BF)
        copy = pltpu.make_async_copy(block_ref.at[:, cols], out_ref.at[:, cols], out_sems.at[part])
        copy.start()
        copies.append(copy)
    for copy in copies:
        copy.wait()


def combine_body(
    in_ref,
    table_hbm,
    lasts_hbm,
    base_hbm,
    own_ref,
    other_ref,
    piece_ref,
    last_ref,
    table_ref,
    lasts_ref,
    base_ref,
    sems,
):
    loads = []
    for n, (source, target) in enumerate(
        ((table_hbm, table_ref), (lasts_hbm, lasts_ref), (base_hbm, base_ref))
    ):
        copy = pltpu.make_async_copy(source, target, sems.at[n])
        copy.start()
        loads.append(copy)
    rows, half = own_ref.shape
    features = 2 * half
    take_pieces(piece_ref, in_ref, features, last_ref, 0)
    for copy in loads:
        copy.wait()
    total = jnp.dot(
        table_ref[...], in_ref[:, :features], preferred_element_type=F32
    ) + jnp.dot(lasts_ref[...], last_ref[...], preferred_element_type=F32)
    total = total[:rows] + total[rows:]
    own_ref[...] = total[:, :half] + base_ref[...]
    other_ref[...] = total[:, half:]


def vmem(count):
    return [pl.BlockSpec(memory_space=pltpu.VMEM)] * count


def hbm(count):
    return [pl.BlockSpec(memory_space=pltpu.HBM)] * count


def in_hbm(x):
    return pltpu.with_memory_space_constraint(x, pltpu.HBM)


def smem():
    return [pl.BlockSpec(memory_space=pltpu.SMEM)]


def per_device(
    stream,
    conv_state,
    recur_state,
    mix_gain,
    branch_weight,
    gate_weight,
    conv_taps,
    recur_map,
    input_map,
    decay_logit,
    out_weight,
    moe_gain,
    route_ids,
    route_weights,
    expert_gate,
    expert_up,
    expert_down,
    dense_gate,
    dense_up,
    dense_down,
    dense_scale,
):
    core = lax.axis_index("tp")
    core_arr = core.astype(jnp.int32).reshape(1)
    seq_count, half = stream.shape
    features = 2 * half
    experts = lax.axis_size("ep")
    own_gate, own_up, own_down = expert_gate[0], expert_up[0], expert_down[0]
    stream_other = swapped(stream)
    branch_near, conv_part, decay = pl.pallas_call(
        warm_body,
        name="warm",
        out_shape=(
            jax.ShapeDtypeStruct((features, half), BF),
            jax.ShapeDtypeStruct((seq_count, half), F32),
            jax.ShapeDtypeStruct((1, half), F32),
        ),
        in_specs=hbm(4),
        out_specs=tuple(vmem(3)),
        scratch_shapes=[
            pltpu.VMEM((3, seq_count, half), BF),
            pltpu.VMEM((4, half), F32),
            pltpu.VMEM((1, half), F32),
            pltpu.SemaphoreType.DMA((4,)),
        ],
        compiler_params=pltpu.CompilerParams(vmem_limit_bytes=8 * MIB),
    )(
        *(
            in_hbm(x)
            for x in (
                branch_weight,
                conv_state.transpose(1, 0, 2),
                conv_taps,
                decay_logit.reshape(1, half),
            )
        )
    )
    branch_in, new_state, mixer_in, out_own = pl.pallas_call(
        mixer_body,
        name="mixer",
        out_shape=(
            pltpu.HBM((seq_count, half), BF),
            pltpu.HBM((seq_count, half), F32),
            jax.ShapeDtypeStruct((seq_count, half), BF),
            jax.ShapeDtypeStruct((half, half), BF),
        ),
        in_specs=smem() + vmem(10) + hbm(2),
        out_specs=tuple(hbm(2) + vmem(2)),
        scratch_shapes=[
            pltpu.VMEM((features, half), BF),
            pltpu.VMEM((seq_count, half), BF),
            pltpu.VMEM((seq_count, half), F32),
            pltpu.SemaphoreType.DMA((4,)),
        ],
        compiler_params=pltpu.CompilerParams(vmem_limit_bytes=14 * MIB),
        cost_estimate=pl.CostEstimate(
            flops=4 * seq_count * features * half,
            transcendentals=6 * seq_count * half,
            bytes_accessed=4 * features * half,
        ),
    )(
        core_arr,
        stream,
        stream_other,
        mix_gain.reshape(1, features),
        branch_near,
        conv_part,
        conv_taps,
        decay,
        recur_map,
        input_map,
        recur_state,
        in_hbm(gate_weight),
        in_hbm(out_weight),
    )
    own_gate, own_up, own_down, mixer_in = lax.optimization_barrier(
        (own_gate, own_up, own_down, mixer_in)
    )
    mixer_other = swapped(mixer_in)
    other_gate, other_up, other_down = swapped(own_gate), swapped(own_up), swapped(own_down)
    part, out_other = pl.pallas_call(
        near_body,
        name="near",
        out_shape=(
            jax.ShapeDtypeStruct((seq_count, half), F32),
            jax.ShapeDtypeStruct((half, half), BF),
        ),
        in_specs=smem() + vmem(2) + hbm(1),
        out_specs=tuple(vmem(2)),
        scratch_shapes=[pltpu.SemaphoreType.DMA],
        compiler_params=pltpu.CompilerParams(vmem_limit_bytes=8 * MIB),
    )(core_arr, mixer_in, out_own, in_hbm(out_weight))
    resid = pl.pallas_call(
        resid_body,
        name="resid",
        out_shape=jax.ShapeDtypeStruct((seq_count, half), BF),
        in_specs=vmem(4),
        out_specs=vmem(1)[0],
        compiler_params=pltpu.CompilerParams(vmem_limit_bytes=8 * MIB),
    )(part, mixer_other, out_other, stream)
    resid_other = swapped(resid)

    block = features + features // MAIN
    count = experts * MAIN
    pieces = pltpu.VMEM((2, count, LANES), F32)
    ids_t, weights_t = route_ids.T, route_weights.T
    payload, normed_two = pl.pallas_call(
        pack_body,
        name="pack",
        out_shape=(
            jax.ShapeDtypeStruct((count, block), BF),
            pltpu.HBM((seq_count, features), BF),
        ),
        in_specs=smem() + vmem(4),
        out_specs=(vmem(1)[0], hbm(1)[0]),
        scratch_shapes=[
            pltpu.VMEM((seq_count, features), BF),
            pieces,
            pltpu.SemaphoreType.DMA,
        ],
        compiler_params=pltpu.CompilerParams(vmem_limit_bytes=14 * MIB),
    )(core_arr, resid, resid_other, moe_gain.reshape(1, features), ids_t)

    incoming = lax.all_to_all(
        payload.reshape(experts, MAIN, block), "ep", split_axis=0, concat_axis=0, tiled=True
    )
    incoming, normed_two, ids_late, weights_late, branch_in, conv_late = lax.optimization_barrier(
        (incoming, normed_two, ids_t, weights_t, branch_in, conv_state)
    )
    new_conv = jnp.concatenate([conv_late[:, 1:], branch_in[:, None]], axis=1)
    incoming = incoming.reshape(count, block)
    table, last = pl.pallas_call(
        table_body,
        name="table",
        out_shape=(
            jax.ShapeDtypeStruct((2 * seq_count, count), BF),
            jax.ShapeDtypeStruct((2 * seq_count, experts), BF),
        ),
        in_specs=smem() + vmem(2),
        out_specs=tuple(vmem(2)),
        compiler_params=pltpu.CompilerParams(vmem_limit_bytes=8 * MIB),
    )(core_arr, ids_late, weights_late)

    own_two, other_two = normed_two[:, :half], normed_two[:, half:]
    whole_two = in_order(core, own_two, other_two)
    dense_hidden = (
        jax.nn.silu(jnp.dot(whole_two, dense_gate, preferred_element_type=F32))
        * jnp.dot(whole_two, dense_up, preferred_element_type=F32)
    ).astype(BF)
    dense_whole = in_order(core, dense_hidden, swapped(dense_hidden))
    dense_out = jnp.dot(dense_whole, dense_down, preferred_element_type=F32).astype(BF)
    base = resid.astype(F32) + dense_scale * dense_out.astype(F32)

    served = pl.pallas_call(
        expert_body,
        name="experts",
        out_shape=pltpu.HBM((count, block), BF),
        in_specs=smem() + vmem(7),
        out_specs=hbm(1)[0],
        scratch_shapes=[
            pltpu.VMEM((count, block), BF),
            pieces,
            pieces,
            pltpu.VMEM((experts * SLOTS, features), BF),
            pltpu.SemaphoreType.DMA((2,)),
        ],
        compiler_params=pltpu.CompilerParams(vmem_limit_bytes=24 * MIB),
    )(
        core_arr,
        incoming,
        own_gate,
        other_gate,
        own_up,
        other_up,
        own_down,
        other_down,
    )

    returned = lax.all_to_all(
        served.reshape(experts, MAIN, block), "ep", split_axis=0, concat_axis=0, tiled=True
    )
    returned, base, new_conv, new_state, table, last = lax.optimization_barrier(
        (returned, base, new_conv, new_state, table, last)
    )
    returned = returned.reshape(count, block)
    sum_own, sum_other = pl.pallas_call(
        combine_body,
        name="combine",
        out_shape=(
            jax.ShapeDtypeStruct((seq_count, half), F32),
            jax.ShapeDtypeStruct((seq_count, half), F32),
        ),
        in_specs=vmem(1) + hbm(3),
        out_specs=tuple(vmem(2)),
        scratch_shapes=[
            pieces,
            pltpu.VMEM((experts, features), BF),
            pltpu.VMEM((2 * seq_count, count), BF),
            pltpu.VMEM((2 * seq_count, experts), BF),
            pltpu.VMEM((seq_count, half), F32),
            pltpu.SemaphoreType.DMA((3,)),
        ],
        compiler_params=pltpu.CompilerParams(vmem_limit_bytes=14 * MIB),
    )(returned, *(in_hbm(x) for x in (table, last, base)))
    result = (sum_own + swapped(sum_other)).astype(BF)
    return (result, new_state, new_conv)


def solution(mesh):
    in_specs = (
        P("ep", "tp"),
        P("ep", None, "tp"),
        P("ep", "tp"),
        P(),
        P(None, "tp"),
        P(None, "tp"),
        P(None, "tp"),
        P("tp", None, None),
        P("tp", None, None),
        P("tp"),
        P(None, "tp"),
        P(),
        P("ep", None),
        P("ep", None),
        P("ep", None, "tp"),
        P("ep", None, "tp"),
        P("ep", None, "tp"),
        P(None, "tp"),
        P(None, "tp"),
        P(None, "tp"),
        P("tp"),
    )
    out_specs = (P("ep", "tp"), P("ep", "tp"), P("ep", None, "tp"))
    return jax.shard_map(
        per_device, mesh=mesh, in_specs=in_specs, out_specs=out_specs, check_vma=False
    )
```

```python
import functools

import jax
import jax.numpy as jnp
from jax import lax
from jax.experimental import pallas as pl
from jax.experimental.pallas import tpu as pltpu
from jax.sharding import PartitionSpec as P


BF = jnp.bfloat16
F32 = jnp.float32
SWAP = [(0, 1), (1, 0)]
MIB = 1024 * 1024
LANES = 128
SLOTS = 9
MAIN = 8
CHUNKS = 4


def swapped(x):
    return lax.ppermute(x, "tp", SWAP)


def in_order(core, own, other):
    return jnp.where(
        core == 0,
        jnp.concatenate([own, other], axis=1),
        jnp.concatenate([other, own], axis=1),
    )


def places(ids, core):
    experts = rows = ids.shape[1]
    expert = lax.broadcasted_iota(jnp.int32, (experts, rows), 0)
    hits = [ids[k : k + 1, :] == expert for k in range(ids.shape[0])]
    chosen = functools.reduce(jnp.logical_or, hits)
    earlier = lax.broadcasted_iota(jnp.int32, (rows, rows), 0) < lax.broadcasted_iota(
        jnp.int32, (rows, rows), 1
    )
    rank = jnp.dot(
        jnp.where(chosen, 1.0, 0.0).astype(BF),
        jnp.where(earlier, 1.0, 0.0).astype(BF),
        preferred_element_type=F32,
    )
    return hits, jnp.where(chosen, rank - (SLOTS * core).astype(F32), -1.0)


def each_slot(values):
    experts = values.shape[0]
    shape = (experts * MAIN, experts)
    row = lax.broadcasted_iota(jnp.int32, shape, 0) // MAIN
    spread = jnp.where(row == lax.broadcasted_iota(jnp.int32, shape, 1), 1.0, 0.0).astype(BF)
    return jnp.dot(spread, values.astype(BF), preferred_element_type=F32)


def slot_number(shape):
    return (lax.broadcasted_iota(jnp.int32, shape, 0) % MAIN).astype(F32)


def put_pieces(piece_ref, values, start, base):
    count = values.shape[0]
    for n in range(values.shape[1] // LANES):
        c, part = divmod(start + n, 2)
        piece_ref[part, pl.ds(base + c, count, stride=MAIN), :] = values[
            :, n * LANES : (n + 1) * LANES
        ]


def take_pieces(piece_ref, block_ref, features, rows_ref, low=0, high=None):
    count = block_ref.shape[0] // MAIN
    piece_ref[0] = block_ref[:, features : features + LANES].astype(F32)
    piece_ref[1] = block_ref[:, features + LANES :].astype(F32)
    for n in range(low // LANES, (high or features) // LANES):
        c, part = divmod(n, 2)
        column = n * LANES - low
        rows_ref[:count, column : column + LANES] = piece_ref[
            part, pl.ds(c, count, stride=MAIN), :
        ].astype(BF)


def route_body(core_ref, ids_ref, table_ref, last_ref):
    _, place = places(ids_ref[...], core_ref[0])
    wide = each_slot(place)
    table_ref[...] = jnp.where(wide == slot_number(wide.shape), 1.0, 0.0).astype(BF)
    last_ref[...] = jnp.where(place == float(MAIN), 1.0, 0.0).astype(BF)


def pack_body(
    core_ref,
    own_ref,
    other_ref,
    gain_ref,
    table_ref,
    last_ref,
    out_ref,
    norm_out_ref,
    norm_ref,
    piece_ref,
    sem,
):
    core = core_ref[0]
    half = own_ref.shape[1]
    features = 2 * half
    own = own_ref[...].astype(F32)
    other = other_ref[...].astype(F32)
    mean = (jnp.sum(own, 1, keepdims=True) + jnp.sum(other, 1, keepdims=True)) / features
    square = (
        jnp.sum(own * own, 1, keepdims=True) + jnp.sum(other * other, 1, keepdims=True)
    ) / features
    scale = lax.rsqrt(square - mean * mean + 1e-05)
    low, high = gain_ref[:, :half], gain_ref[:, half:]
    gain_own = jnp.where(core == 0, low, high)
    gain_other = jnp.where(core == 0, high, low)
    norm_ref[:, :half] = ((own - mean) * scale * gain_own).astype(BF)
    norm_ref[:, half:] = ((other - mean) * scale * gain_other).astype(BF)
    norm_copy = pltpu.make_async_copy(norm_ref, norm_out_ref, sem)
    norm_copy.start()
    rows = norm_ref[...]
    put_pieces(piece_ref, jnp.dot(last_ref[...], rows, preferred_element_type=F32), 0, 0)
    out_ref[:, :features] = jnp.dot(table_ref[...], rows, preferred_element_type=F32).astype(BF)
    out_ref[:, features : features + LANES] = piece_ref[0].astype(BF)
    out_ref[:, features + LANES :] = piece_ref[1].astype(BF)
    norm_copy.wait()


def start_all(pairs, sems):
    copies = [
        pltpu.make_async_copy(source, target, sems.at[n])
        for n, (source, target) in enumerate(pairs)
    ]
    for copy in copies:
        copy.start()
    return copies


def wait_all(copies):
    for copy in copies:
        copy.wait()


def warm_body(
    weight_hbm,
    state_hbm,
    taps_hbm,
    logit_hbm,
    weight_ref,
    conv_ref,
    decay_ref,
    state_ref,
    taps_ref,
    logit_ref,
    sems,
):
    copies = start_all(
        (
            (state_hbm, state_ref),
            (taps_hbm, taps_ref),
            (logit_hbm, logit_ref),
            (weight_hbm, weight_ref),
        ),
        sems,
    )
    wait_all(copies[:3])
    conv = state_ref[0].astype(F32) * taps_ref[0:1, :]
    for offset in range(1, 3):
        conv = conv + state_ref[offset].astype(F32) * taps_ref[offset : offset + 1, :]
    conv_ref[...] = conv
    decay_ref[...] = -8.0 * jax.nn.softplus(-logit_ref[...])
    wait_all(copies[3:])


def near_body(core_ref, mixed_ref, weight_ref, weight_hbm, part_ref, other_ref, sem):
    half = mixed_ref.shape[1]
    second = pl.ds(pl.multiple_of((1 - core_ref[0]) * half, half), half)
    copy = pltpu.make_async_copy(weight_hbm.at[second, :], other_ref, sem)
    copy.start()
    part_ref[...] = jnp.dot(mixed_ref[...], weight_ref[...], preferred_element_type=F32)
    copy.wait()


def resid_body(part_ref, mixed_ref, weight_ref, stream_ref, out_ref):
    mixer_out = part_ref[...] + jnp.dot(
        mixed_ref[...], weight_ref[...], preferred_element_type=F32
    )
    out_ref[...] = (stream_ref[...].astype(F32) + mixer_out.astype(BF).astype(F32)).astype(BF)


def mixer_body(
    core_ref,
    own_ref,
    other_ref,
    gain_ref,
    branch_ref,
    conv_ref,
    taps_ref,
    decay_ref,
    recur_ref,
    input_ref,
    state_ref,
    gate_hbm,
    out_hbm,
    branch_out_hbm,
    state_out_hbm,
    mixed_ref,
    weight_ref,
    gate_ref,
    branch_out_ref,
    state_out_ref,
    sems,
):
    core = core_ref[0]
    half = own_ref.shape[1]
    features = 2 * half
    first = pl.ds(pl.multiple_of(core * half, half), half)
    second = pl.ds(pl.multiple_of((1 - core) * half, half), half)
    copies = start_all(((gate_hbm, gate_ref), (out_hbm.at[first, :], weight_ref)), sems)
    own = own_ref[...].astype(F32)
    other = other_ref[...].astype(F32)
    mean = (jnp.sum(own, 1, keepdims=True) + jnp.sum(other, 1, keepdims=True)) / features
    square = (
        jnp.sum(own * own, 1, keepdims=True) + jnp.sum(other * other, 1, keepdims=True)
    ) / features
    scale = lax.rsqrt(square - mean * mean + 1e-05)
    low, high = gain_ref[:, :half], gain_ref[:, half:]
    own = ((own - mean) * scale * jnp.where(core == 0, low, high)).astype(BF)
    other = ((other - mean) * scale * jnp.where(core == 0, high, low)).astype(BF)

    def product(weight):
        return (
            jnp.dot(own, weight[first, :], preferred_element_type=F32)
            + jnp.dot(other, weight[second, :], preferred_element_type=F32)
        ).astype(BF)

    branch = product(branch_ref)
    branch_out_ref[...] = branch
    conv = (conv_ref[...] + branch.astype(F32) * taps_ref[3:4, :]).astype(BF)
    width = recur_ref.shape[1]
    recur, drive = (
        jnp.concatenate(
            [
                jnp.dot(
                    conv[:, n * width : (n + 1) * width], maps[n], preferred_element_type=F32
                )
                for n in range(maps.shape[0])
            ],
            axis=1,
        )
        for maps in (recur_ref, input_ref)
    )
    log_decay = jax.nn.sigmoid(recur) * decay_ref[...]
    turn = jnp.tanh(log_decay)
    kept = jnp.sqrt(-2.0 * turn / (1.0 - turn))
    driven = kept * (jax.nn.sigmoid(drive) * conv.astype(F32))
    state = jnp.exp(log_decay) * state_ref[...] + driven
    state_out_ref[...] = state
    branch_copy = pltpu.make_async_copy(branch_out_ref, branch_out_hbm, sems.at[2])
    branch_copy.start()
    state_copy = pltpu.make_async_copy(state_out_ref, state_out_hbm, sems.at[3])
    state_copy.start()
    wait_all(copies[:1])
    mixed_ref[...] = (jax.nn.gelu(product(gate_ref).astype(F32)) * state).astype(BF)
    wait_all([*copies[1:], branch_copy, state_copy])


def table_body(core_ref, ids_ref, weights_ref, table_ref, last_ref):
    rows = ids_ref.shape[1]
    hits, place = places(ids_ref[...], core_ref[0])
    weight = functools.reduce(
        jnp.add,
        [jnp.where(hit, weights_ref[k : k + 1, :], 0.0) for k, hit in enumerate(hits)],
    )
    high = weight.astype(BF).astype(F32)
    low = (weight - high).astype(BF).astype(F32)
    wide = each_slot(place)
    match = wide == slot_number(wide.shape)
    for n, part in enumerate((high, low)):
        span = slice(n * rows, (n + 1) * rows)
        table_ref[span, :] = jnp.transpose(jnp.where(match, each_slot(part), 0.0)).astype(BF)
        last_ref[span, :] = jnp.transpose(jnp.where(place == float(MAIN), part, 0.0)).astype(BF)


def expert_body(
    core_ref,
    in_ref,
    gate_ref,
    gate2_ref,
    up_ref,
    up2_ref,
    down_ref,
    down2_ref,
    out_ref,
    block_ref,
    piece_ref,
    take_ref,
    rows_ref,
    out_sems,
):
    core = core_ref[0]
    features, units = gate_ref.shape
    half = features // 2
    first = pl.ds(pl.multiple_of(core * half, half), half)
    second = pl.ds(pl.multiple_of((1 - core) * half, half), half)
    unit_own = pl.ds(pl.multiple_of(core * units, units), units)
    unit_other = pl.ds(pl.multiple_of((1 - core) * units, units), units)
    count = in_ref.shape[0]
    extra = count // MAIN
    take_pieces(take_ref, in_ref, features, rows_ref)
    rows_ref[extra:, :] = in_ref[:, :features]

    def product(weight):
        return jnp.dot(
            rows_ref[:, :half], weight[first, :], preferred_element_type=F32
        ) + jnp.dot(rows_ref[:, half:], weight[second, :], preferred_element_type=F32)

    def hidden(gate, up):
        return (jax.nn.silu(product(gate)) * product(up)).astype(BF)

    hid_own = hidden(gate_ref, up_ref)
    hid_other = hidden(gate2_ref, up2_ref)

    def served(down, span):
        return jnp.dot(hid_own[span], down[unit_own, :], preferred_element_type=F32) + jnp.dot(
            hid_other[span], down[unit_other, :], preferred_element_type=F32
        )

    own = served(down_ref, slice(None))
    put_pieces(piece_ref, own[:extra], 0, 0)
    block_ref[:, :half] = own[extra:].astype(BF)
    copies = [
        pltpu.make_async_copy(block_ref.at[:, :half], out_ref.at[:, :half], out_sems.at[CHUNKS])
    ]
    copies[0].start()
    step = count // CHUNKS
    for n in range(CHUNKS):
        low = extra + n * step if n else 0
        other = served(down2_ref, slice(low, extra + (n + 1) * step))
        if n == 0:
            put_pieces(piece_ref, other[:extra], half // LANES, 0)
            other = other[extra:]
        span = slice(n * step, (n + 1) * step)
        block_ref[span, half:features] = other.astype(BF)
        block_ref[span, features : features + LANES] = piece_ref[0, span].astype(BF)
        block_ref[span, features + LANES :] = piece_ref[1, span].astype(BF)
        copy = pltpu.make_async_copy(
            block_ref.at[span, half:], out_ref.at[span, half:], out_sems.at[n]
        )
        copy.start()
        copies.append(copy)
    wait_all(copies)


def half_sum(in_ref, table_ref, lasts_ref, piece_ref, last_ref, low, high, features, copies=()):
    take_pieces(piece_ref, in_ref, features, last_ref, low, high)
    wait_all(copies)
    total = jnp.dot(
        table_ref[...], in_ref[:, low:high], preferred_element_type=F32
    ) + jnp.dot(lasts_ref[...], last_ref[...], preferred_element_type=F32)
    rows = total.shape[0] // 2
    return total[:rows] + total[rows:]


def combine_body(
    in_ref, table_hbm, lasts_hbm, other_ref, table_ref, lasts_ref, piece_ref, last_ref, sems
):
    copies = start_all(((table_hbm, table_ref), (lasts_hbm, lasts_ref)), sems)
    half = other_ref.shape[1]
    other_ref[...] = half_sum(
        in_ref, table_ref, lasts_ref, piece_ref, last_ref, half, 2 * half, 2 * half, copies
    ).astype(BF)


def finish_body(
    in_ref, table_ref, lasts_ref, base_hbm, own_ref, piece_ref, last_ref, base_ref, sem
):
    copy = pltpu.make_async_copy(base_hbm, base_ref, sem)
    copy.start()
    half = own_ref.shape[1]
    total = half_sum(in_ref, table_ref, lasts_ref, piece_ref, last_ref, 0, half, 2 * half)
    copy.wait()
    own_ref[...] = total + base_ref[...]


def vmem(count):
    return [pl.BlockSpec(memory_space=pltpu.VMEM)] * count


def hbm(count):
    return [pl.BlockSpec(memory_space=pltpu.HBM)] * count


def in_hbm(x):
    return pltpu.with_memory_space_constraint(x, pltpu.HBM)


def smem():
    return [pl.BlockSpec(memory_space=pltpu.SMEM)]


def per_device(
    stream,
    conv_state,
    recur_state,
    mix_gain,
    branch_weight,
    gate_weight,
    conv_taps,
    recur_map,
    input_map,
    decay_logit,
    out_weight,
    moe_gain,
    route_ids,
    route_weights,
    expert_gate,
    expert_up,
    expert_down,
    dense_gate,
    dense_up,
    dense_down,
    dense_scale,
):
    core = lax.axis_index("tp")
    core_arr = core.astype(jnp.int32).reshape(1)
    seq_count, half = stream.shape
    features = 2 * half
    experts = lax.axis_size("ep")
    own_gate, own_up, own_down = expert_gate[0], expert_up[0], expert_down[0]
    stream_other = swapped(stream)
    branch_near, conv_part, decay = pl.pallas_call(
        warm_body,
        name="warm",
        out_shape=(
            jax.ShapeDtypeStruct((features, half), BF),
            jax.ShapeDtypeStruct((seq_count, half), F32),
            jax.ShapeDtypeStruct((1, half), F32),
        ),
        in_specs=hbm(4),
        out_specs=tuple(vmem(3)),
        scratch_shapes=[
            pltpu.VMEM((3, seq_count, half), BF),
            pltpu.VMEM((4, half), F32),
            pltpu.VMEM((1, half), F32),
            pltpu.SemaphoreType.DMA((4,)),
        ],
        compiler_params=pltpu.CompilerParams(vmem_limit_bytes=8 * MIB),
    )(
        *(
            in_hbm(x)
            for x in (
                branch_weight,
                conv_state.transpose(1, 0, 2),
                conv_taps,
                decay_logit.reshape(1, half),
            )
        )
    )
    branch_in, new_state, mixer_in, out_own = pl.pallas_call(
        mixer_body,
        name="mixer",
        out_shape=(
            pltpu.HBM((seq_count, half), BF),
            pltpu.HBM((seq_count, half), F32),
            jax.ShapeDtypeStruct((seq_count, half), BF),
            jax.ShapeDtypeStruct((half, half), BF),
        ),
        in_specs=smem() + vmem(10) + hbm(2),
        out_specs=tuple(hbm(2) + vmem(2)),
        scratch_shapes=[
            pltpu.VMEM((features, half), BF),
            pltpu.VMEM((seq_count, half), BF),
            pltpu.VMEM((seq_count, half), F32),
            pltpu.SemaphoreType.DMA((4,)),
        ],
        compiler_params=pltpu.CompilerParams(vmem_limit_bytes=14 * MIB),
        cost_estimate=pl.CostEstimate(
            flops=4 * seq_count * features * half,
            transcendentals=6 * seq_count * half,
            bytes_accessed=4 * features * half,
        ),
    )(
        core_arr,
        stream,
        stream_other,
        mix_gain.reshape(1, features),
        branch_near,
        conv_part,
        conv_taps,
        decay,
        recur_map,
        input_map,
        recur_state,
        in_hbm(gate_weight),
        in_hbm(out_weight),
    )
    own_gate, own_up, own_down, mixer_in = lax.optimization_barrier(
        (own_gate, own_up, own_down, mixer_in)
    )
    mixer_other = swapped(mixer_in)
    other_gate, other_up, other_down = swapped(own_gate), swapped(own_up), swapped(own_down)
    part, out_other = pl.pallas_call(
        near_body,
        name="near",
        out_shape=(
            jax.ShapeDtypeStruct((seq_count, half), F32),
            jax.ShapeDtypeStruct((half, half), BF),
        ),
        in_specs=smem() + vmem(2) + hbm(1),
        out_specs=tuple(vmem(2)),
        scratch_shapes=[pltpu.SemaphoreType.DMA],
        compiler_params=pltpu.CompilerParams(vmem_limit_bytes=8 * MIB),
    )(core_arr, mixer_in, out_own, in_hbm(out_weight))
    resid = pl.pallas_call(
        resid_body,
        name="resid",
        out_shape=jax.ShapeDtypeStruct((seq_count, half), BF),
        in_specs=vmem(4),
        out_specs=vmem(1)[0],
        compiler_params=pltpu.CompilerParams(vmem_limit_bytes=8 * MIB),
    )(part, mixer_other, out_other, stream)
    ids_t, weights_t = route_ids.T, route_weights.T
    count = experts * MAIN
    resid_other = swapped(resid)
    send_table, send_last = pl.pallas_call(
        route_body,
        name="route",
        out_shape=(
            jax.ShapeDtypeStruct((count, seq_count), BF),
            jax.ShapeDtypeStruct((experts, seq_count), BF),
        ),
        in_specs=smem() + vmem(1),
        out_specs=tuple(vmem(2)),
        compiler_params=pltpu.CompilerParams(vmem_limit_bytes=6 * MIB),
    )(core_arr, ids_t)

    block = features + features // MAIN
    pieces = pltpu.VMEM((2, count, LANES), F32)
    payload, normed_two = pl.pallas_call(
        pack_body,
        name="pack",
        out_shape=(
            jax.ShapeDtypeStruct((count, block), BF),
            pltpu.HBM((seq_count, features), BF),
        ),
        in_specs=smem() + vmem(5),
        out_specs=(vmem(1)[0], hbm(1)[0]),
        scratch_shapes=[
            pltpu.VMEM((seq_count, features), BF),
            pieces,
            pltpu.SemaphoreType.DMA,
        ],
        compiler_params=pltpu.CompilerParams(vmem_limit_bytes=14 * MIB),
    )(core_arr, resid, resid_other, moe_gain.reshape(1, features), send_table, send_last)

    incoming = lax.all_to_all(
        payload.reshape(experts, MAIN, block), "ep", split_axis=0, concat_axis=0, tiled=True
    )
    incoming, normed_two, ids_late, weights_late, branch_in, conv_late = lax.optimization_barrier(
        (incoming, normed_two, ids_t, weights_t, branch_in, conv_state)
    )
    new_conv = jnp.concatenate([conv_late[:, 1:], branch_in[:, None]], axis=1)
    incoming = incoming.reshape(count, block)
    table, last = pl.pallas_call(
        table_body,
        name="table",
        out_shape=(
            jax.ShapeDtypeStruct((2 * seq_count, count), BF),
            jax.ShapeDtypeStruct((2 * seq_count, experts), BF),
        ),
        in_specs=smem() + vmem(2),
        out_specs=tuple(vmem(2)),
        compiler_params=pltpu.CompilerParams(vmem_limit_bytes=8 * MIB),
    )(core_arr, ids_late, weights_late)

    own_two, other_two = normed_two[:, :half], normed_two[:, half:]
    whole_two = in_order(core, own_two, other_two)
    dense_hidden = (
        jax.nn.silu(jnp.dot(whole_two, dense_gate, preferred_element_type=F32))
        * jnp.dot(whole_two, dense_up, preferred_element_type=F32)
    ).astype(BF)
    dense_whole = in_order(core, dense_hidden, swapped(dense_hidden))
    dense_out = jnp.dot(dense_whole, dense_down, preferred_element_type=F32).astype(BF)
    base = resid.astype(F32) + dense_scale * dense_out.astype(F32)

    served = pl.pallas_call(
        expert_body,
        name="experts",
        out_shape=pltpu.HBM((count, block), BF),
        in_specs=smem() + vmem(7),
        out_specs=hbm(1)[0],
        scratch_shapes=[
            pltpu.VMEM((count, block), BF),
            pieces,
            pieces,
            pltpu.VMEM((experts * SLOTS, features), BF),
            pltpu.SemaphoreType.DMA((CHUNKS + 1,)),
        ],
        compiler_params=pltpu.CompilerParams(vmem_limit_bytes=24 * MIB),
    )(
        core_arr,
        incoming,
        own_gate,
        other_gate,
        own_up,
        other_up,
        own_down,
        other_down,
    )

    returned = lax.all_to_all(
        served.reshape(experts, MAIN, block), "ep", split_axis=0, concat_axis=0, tiled=True
    )
    returned, base, new_conv, new_state, table, last = lax.optimization_barrier(
        (returned, base, new_conv, new_state, table, last)
    )
    returned = returned.reshape(count, block)
    sum_other, table, last = pl.pallas_call(
        combine_body,
        name="combine",
        out_shape=(
            jax.ShapeDtypeStruct((seq_count, half), BF),
            jax.ShapeDtypeStruct(table.shape, BF),
            jax.ShapeDtypeStruct(last.shape, BF),
        ),
        in_specs=vmem(1) + hbm(2),
        out_specs=tuple(vmem(3)),
        scratch_shapes=[
            pieces,
            pltpu.VMEM((experts, half), BF),
            pltpu.SemaphoreType.DMA((2,)),
        ],
        compiler_params=pltpu.CompilerParams(vmem_limit_bytes=10 * MIB),
    )(returned, in_hbm(table), in_hbm(last))
    sum_received = swapped(sum_other)
    sum_own = pl.pallas_call(
        finish_body,
        name="finish",
        out_shape=jax.ShapeDtypeStruct((seq_count, half), F32),
        in_specs=vmem(3) + hbm(1),
        out_specs=vmem(1)[0],
        scratch_shapes=[
            pieces,
            pltpu.VMEM((experts, half), BF),
            pltpu.VMEM((seq_count, half), F32),
            pltpu.SemaphoreType.DMA,
        ],
        compiler_params=pltpu.CompilerParams(vmem_limit_bytes=10 * MIB),
    )(returned, table, last, in_hbm(base))
    result = (sum_own + sum_received.astype(F32)).astype(BF)
    return (result, new_state, new_conv)


def solution(mesh):
    in_specs = (
        P("ep", "tp"),
        P("ep", None, "tp"),
        P("ep", "tp"),
        P(),
        P(None, "tp"),
        P(None, "tp"),
        P(None, "tp"),
        P("tp", None, None),
        P("tp", None, None),
        P("tp"),
        P(None, "tp"),
        P(),
        P("ep", None),
        P("ep", None),
        P("ep", None, "tp"),
        P("ep", None, "tp"),
        P("ep", None, "tp"),
        P(None, "tp"),
        P(None, "tp"),
        P(None, "tp"),
        P("tp"),
    )
    out_specs = (P("ep", "tp"), P("ep", "tp"), P("ep", None, "tp"))
    return jax.shard_map(
        per_device, mesh=mesh, in_specs=in_specs, out_specs=out_specs, check_vma=False
    )
```

```python
import functools

import jax
import jax.numpy as jnp
from jax import lax
from jax.experimental import pallas as pl
from jax.experimental.pallas import tpu as pltpu
from jax.sharding import PartitionSpec as P


BF = jnp.bfloat16
F32 = jnp.float32
SWAP = [(0, 1), (1, 0)]
MIB = 1024 * 1024
LANES = 128
SLOTS = 9
MAIN = 8


def swapped(x):
    return lax.ppermute(x, "tp", SWAP)


def places(ids, core):
    experts = rows = ids.shape[1]
    expert = lax.broadcasted_iota(jnp.int32, (experts, rows), 0)
    hits = [ids[k : k + 1, :] == expert for k in range(ids.shape[0])]
    chosen = functools.reduce(jnp.logical_or, hits)
    earlier = lax.broadcasted_iota(jnp.int32, (rows, rows), 0) < lax.broadcasted_iota(
        jnp.int32, (rows, rows), 1
    )
    rank = jnp.dot(
        jnp.where(chosen, 1.0, 0.0).astype(BF),
        jnp.where(earlier, 1.0, 0.0).astype(BF),
        preferred_element_type=F32,
    )
    return hits, jnp.where(chosen, rank - (SLOTS * core).astype(F32), -1.0)


def each_slot(values):
    experts = values.shape[0]
    shape = (experts * MAIN, experts)
    row = lax.broadcasted_iota(jnp.int32, shape, 0) // MAIN
    spread = jnp.where(row == lax.broadcasted_iota(jnp.int32, shape, 1), 1.0, 0.0).astype(BF)
    return jnp.dot(spread, values.astype(BF), preferred_element_type=F32)


def slot_number(shape):
    return (lax.broadcasted_iota(jnp.int32, shape, 0) % MAIN).astype(F32)


def put_pieces(piece_ref, values, start, base):
    count = values.shape[0]
    for n in range(values.shape[1] // LANES):
        c, part = divmod(start + n, 2)
        piece_ref[part, pl.ds(base + c, count, stride=MAIN), :] = values[
            :, n * LANES : (n + 1) * LANES
        ]


def take_pieces(piece_ref, block_ref, features, rows_ref, low=0, high=None):
    count = block_ref.shape[0] // MAIN
    piece_ref[0] = block_ref[:, features : features + LANES].astype(F32)
    piece_ref[1] = block_ref[:, features + LANES :].astype(F32)
    for n in range(low // LANES, (high or features) // LANES):
        c, part = divmod(n, 2)
        column = n * LANES - low
        rows_ref[:count, column : column + LANES] = piece_ref[
            part, pl.ds(c, count, stride=MAIN), :
        ].astype(BF)


def route_body(
    core_ref, ids_ref, weights_ref, table_ref, last_ref, back_table_ref, back_last_ref
):
    rows = ids_ref.shape[1]
    hits, place = places(ids_ref[...], core_ref[0])
    wide = each_slot(place)
    match = wide == slot_number(wide.shape)
    table_ref[...] = jnp.where(match, 1.0, 0.0).astype(BF)
    last_ref[...] = jnp.where(place == float(MAIN), 1.0, 0.0).astype(BF)
    weight = functools.reduce(
        jnp.add,
        [jnp.where(hit, weights_ref[k : k + 1, :], 0.0) for k, hit in enumerate(hits)],
    )
    high = weight.astype(BF).astype(F32)
    low = (weight - high).astype(BF).astype(F32)
    for n, part in enumerate((high, low)):
        span = slice(n * rows, (n + 1) * rows)
        back_table_ref[span, :] = jnp.transpose(jnp.where(match, each_slot(part), 0.0)).astype(BF)
        back_last_ref[span, :] = jnp.transpose(
            jnp.where(place == float(MAIN), part, 0.0)
        ).astype(BF)


def pack_body(
    core_ref,
    own_ref,
    other_ref,
    gain_ref,
    table_ref,
    last_ref,
    out_ref,
    norm_ref,
    piece_ref,
):
    core = core_ref[0]
    half = own_ref.shape[1]
    features = 2 * half
    own = own_ref[...].astype(F32)
    other = other_ref[...].astype(F32)
    mean = (jnp.sum(own, 1, keepdims=True) + jnp.sum(other, 1, keepdims=True)) / features
    square = (
        jnp.sum(own * own, 1, keepdims=True) + jnp.sum(other * other, 1, keepdims=True)
    ) / features
    scale = lax.rsqrt(square - mean * mean + 1e-05)
    low, high = gain_ref[:, :half], gain_ref[:, half:]
    gain_own = jnp.where(core == 0, low, high)
    gain_other = jnp.where(core == 0, high, low)
    norm_ref[:, :half] = ((own - mean) * scale * gain_own).astype(BF)
    norm_ref[:, half:] = ((other - mean) * scale * gain_other).astype(BF)
    rows = norm_ref[...]
    put_pieces(piece_ref, jnp.dot(last_ref[...], rows, preferred_element_type=F32), 0, 0)
    out_ref[:, :features] = jnp.dot(table_ref[...], rows, preferred_element_type=F32).astype(BF)
    out_ref[:, features : features + LANES] = piece_ref[0].astype(BF)
    out_ref[:, features + LANES :] = piece_ref[1].astype(BF)


def start_all(pairs, sems):
    copies = [
        pltpu.make_async_copy(source, target, sems.at[n])
        for n, (source, target) in enumerate(pairs)
    ]
    for copy in copies:
        copy.start()
    return copies


def wait_all(copies):
    for copy in copies:
        copy.wait()


def warm_body(
    weight_hbm,
    state_hbm,
    taps_hbm,
    logit_hbm,
    weight_ref,
    conv_ref,
    decay_ref,
    state_ref,
    taps_ref,
    logit_ref,
    sems,
):
    copies = start_all(
        (
            (state_hbm, state_ref),
            (taps_hbm, taps_ref),
            (logit_hbm, logit_ref),
            (weight_hbm, weight_ref),
        ),
        sems,
    )
    wait_all(copies[:3])
    conv = state_ref[0].astype(F32) * taps_ref[0:1, :]
    for offset in range(1, 3):
        conv = conv + state_ref[offset].astype(F32) * taps_ref[offset : offset + 1, :]
    conv_ref[...] = conv
    decay_ref[...] = -8.0 * jax.nn.softplus(-logit_ref[...])
    wait_all(copies[3:])


def near_body(core_ref, mixed_ref, weight_ref, weight_hbm, part_ref, other_ref, sem):
    half = mixed_ref.shape[1]
    second = pl.ds(pl.multiple_of((1 - core_ref[0]) * half, half), half)
    copy = pltpu.make_async_copy(weight_hbm.at[second, :], other_ref, sem)
    copy.start()
    part_ref[...] = jnp.dot(mixed_ref[...], weight_ref[...], preferred_element_type=F32)
    copy.wait()


def resid_body(part_ref, mixed_ref, weight_ref, stream_ref, out_ref):
    mixer_out = part_ref[...] + jnp.dot(
        mixed_ref[...], weight_ref[...], preferred_element_type=F32
    )
    out_ref[...] = (stream_ref[...].astype(F32) + mixer_out.astype(BF).astype(F32)).astype(BF)


def mixer_body(
    core_ref,
    own_ref,
    other_ref,
    gain_ref,
    branch_ref,
    conv_ref,
    taps_ref,
    decay_ref,
    recur_ref,
    input_ref,
    state_ref,
    gate_hbm,
    out_hbm,
    new_conv_hbm,
    new_state_hbm,
    mixed_ref,
    weight_ref,
    gate_ref,
    branch_out_ref,
    state_out_ref,
    sems,
):
    core = core_ref[0]
    half = own_ref.shape[1]
    features = 2 * half
    first = pl.ds(pl.multiple_of(core * half, half), half)
    second = pl.ds(pl.multiple_of((1 - core) * half, half), half)
    copies = start_all(
        (
            (gate_hbm, gate_ref),
            (out_hbm.at[first, :], weight_ref),
        ),
        sems,
    )
    own = own_ref[...].astype(F32)
    other = other_ref[...].astype(F32)
    mean = (jnp.sum(own, 1, keepdims=True) + jnp.sum(other, 1, keepdims=True)) / features
    square = (
        jnp.sum(own * own, 1, keepdims=True) + jnp.sum(other * other, 1, keepdims=True)
    ) / features
    scale = lax.rsqrt(square - mean * mean + 1e-05)
    low, high = gain_ref[:, :half], gain_ref[:, half:]
    own = ((own - mean) * scale * jnp.where(core == 0, low, high)).astype(BF)
    other = ((other - mean) * scale * jnp.where(core == 0, high, low)).astype(BF)

    def product(weight):
        return (
            jnp.dot(own, weight[first, :], preferred_element_type=F32)
            + jnp.dot(other, weight[second, :], preferred_element_type=F32)
        ).astype(BF)

    branch = product(branch_ref)
    branch_out_ref[...] = branch
    conv = (conv_ref[...] + branch.astype(F32) * taps_ref[3:4, :]).astype(BF)
    width = recur_ref.shape[1]
    recur, drive = (
        jnp.concatenate(
            [
                jnp.dot(
                    conv[:, n * width : (n + 1) * width], maps[n], preferred_element_type=F32
                )
                for n in range(maps.shape[0])
            ],
            axis=1,
        )
        for maps in (recur_ref, input_ref)
    )
    log_decay = jax.nn.sigmoid(recur) * decay_ref[...]
    turn = jnp.tanh(log_decay)
    kept = jnp.sqrt(-2.0 * turn / (1.0 - turn))
    driven = kept * (jax.nn.sigmoid(drive) * conv.astype(F32))
    state = jnp.exp(log_decay) * state_ref[...] + driven
    state_out_ref[...] = state
    branch_copy = pltpu.make_async_copy(branch_out_ref, new_conv_hbm.at[2], sems.at[2])
    branch_copy.start()
    state_copy = pltpu.make_async_copy(state_out_ref, new_state_hbm, sems.at[3])
    state_copy.start()
    wait_all(copies[:1])
    mixed_ref[...] = (jax.nn.gelu(product(gate_ref).astype(F32)) * state).astype(BF)
    wait_all([*copies[1:], branch_copy, state_copy])


def expert_body(
    core_ref,
    in_ref,
    gate_ref,
    gate2_ref,
    up_ref,
    up2_ref,
    down_ref,
    down2_ref,
    normed_ref,
    dense_gate_ref,
    dense_up_ref,
    old_conv_ref,
    dense_down_hbm,
    dense_scale_hbm,
    conv_begun_hbm,
    out_ref,
    dense_ref,
    dense_down_ref,
    dense_scale_ref,
    new_conv_hbm,
    piece_ref,
    take_ref,
    rows_ref,
    sems,
):
    copies = start_all(
        (
            (dense_down_hbm, dense_down_ref),
            (dense_scale_hbm, dense_scale_ref),
            (old_conv_ref.at[pl.ds(1, 2)], new_conv_hbm.at[pl.ds(0, 2)]),
        ),
        sems,
    )
    core = core_ref[0]
    features, units = gate_ref.shape
    half = features // 2
    first = pl.ds(pl.multiple_of(core * half, half), half)
    second = pl.ds(pl.multiple_of((1 - core) * half, half), half)
    unit_own = pl.ds(pl.multiple_of(core * units, units), units)
    unit_other = pl.ds(pl.multiple_of((1 - core) * units, units), units)
    count = in_ref.shape[0]
    extra = count // MAIN
    take_pieces(take_ref, in_ref, features, rows_ref)
    rows_ref[extra:, :] = in_ref[:, :features]

    def hidden(rows, gate, up):
        gated, raised = (
            jnp.dot(rows[:, :half], weight[first, :], preferred_element_type=F32)
            + jnp.dot(rows[:, half:], weight[second, :], preferred_element_type=F32)
            for weight in (gate, up)
        )
        return (jax.nn.silu(gated) * raised).astype(BF)

    dense_ref[...] = hidden(normed_ref, dense_gate_ref, dense_up_ref)
    hid_own = hidden(rows_ref, gate_ref, up_ref)
    hid_other = hidden(rows_ref, gate2_ref, up2_ref)

    def served(down, span):
        return jnp.dot(hid_own[span], down[unit_own, :], preferred_element_type=F32) + jnp.dot(
            hid_other[span], down[unit_other, :], preferred_element_type=F32
        )

    for part, down in enumerate((down_ref, down2_ref)):
        values = served(down, slice(None))
        put_pieces(piece_ref, values[:extra], part * (half // LANES), 0)
        out_ref[:, part * half : (part + 1) * half] = values[extra:].astype(BF)
    out_ref[:, features : features + LANES] = piece_ref[0].astype(BF)
    out_ref[:, features + LANES :] = piece_ref[1].astype(BF)
    wait_all(copies)


def half_sum(in_ref, table_ref, lasts_ref, piece_ref, last_ref, low, high, features):
    take_pieces(piece_ref, in_ref, features, last_ref, low, high)
    total = jnp.dot(
        table_ref[...], in_ref[:, low:high], preferred_element_type=F32
    ) + jnp.dot(lasts_ref[...], last_ref[...], preferred_element_type=F32)
    rows = total.shape[0] // 2
    return total[:rows] + total[rows:]


def combine_body(in_ref, table_ref, lasts_ref, other_ref, piece_ref, last_ref):
    half = other_ref.shape[1]
    other_ref[...] = half_sum(
        in_ref, table_ref, lasts_ref, piece_ref, last_ref, half, 2 * half, 2 * half
    ).astype(BF)


def finish_body(
    core_ref,
    in_ref,
    table_ref,
    lasts_ref,
    resid_ref,
    own_hid_ref,
    other_hid_ref,
    down_ref,
    scale_ref,
    own_ref,
    piece_ref,
    last_ref,
):
    core = core_ref[0]
    half = own_ref.shape[1]
    units = own_hid_ref.shape[1]
    unit_own = pl.ds(pl.multiple_of(core * units, units), units)
    unit_other = pl.ds(pl.multiple_of((1 - core) * units, units), units)
    dense = jnp.dot(own_hid_ref[...], down_ref[unit_own, :], preferred_element_type=F32) + jnp.dot(
        other_hid_ref[...], down_ref[unit_other, :], preferred_element_type=F32
    )
    base = resid_ref[...].astype(F32) + scale_ref[...] * dense.astype(BF).astype(F32)
    own_ref[...] = base + half_sum(
        in_ref, table_ref, lasts_ref, piece_ref, last_ref, 0, half, 2 * half
    )


def vmem(count):
    return [pl.BlockSpec(memory_space=pltpu.VMEM)] * count


def hbm(count):
    return [pl.BlockSpec(memory_space=pltpu.HBM)] * count


def in_hbm(x):
    return pltpu.with_memory_space_constraint(x, pltpu.HBM)


def smem():
    return [pl.BlockSpec(memory_space=pltpu.SMEM)]


def per_device(
    stream,
    conv_state,
    recur_state,
    mix_gain,
    branch_weight,
    gate_weight,
    conv_taps,
    recur_map,
    input_map,
    decay_logit,
    out_weight,
    moe_gain,
    route_ids,
    route_weights,
    expert_gate,
    expert_up,
    expert_down,
    dense_gate,
    dense_up,
    dense_down,
    dense_scale,
):
    core = lax.axis_index("tp")
    core_arr = core.astype(jnp.int32).reshape(1)
    seq_count, half = stream.shape
    features = 2 * half
    experts = lax.axis_size("ep")
    own_gate, own_up, own_down = expert_gate[0], expert_up[0], expert_down[0]
    stream_other = swapped(stream)
    branch_near, conv_part, decay, old_conv = pl.pallas_call(
        warm_body,
        name="warm",
        out_shape=(
            jax.ShapeDtypeStruct((features, half), BF),
            jax.ShapeDtypeStruct((seq_count, half), F32),
            jax.ShapeDtypeStruct((1, half), F32),
            jax.ShapeDtypeStruct((3, seq_count, half), BF),
        ),
        in_specs=hbm(4),
        out_specs=tuple(vmem(4)),
        scratch_shapes=[
            pltpu.VMEM((4, half), F32),
            pltpu.VMEM((1, half), F32),
            pltpu.SemaphoreType.DMA((4,)),
        ],
        compiler_params=pltpu.CompilerParams(vmem_limit_bytes=8 * MIB),
    )(
        *(
            in_hbm(x)
            for x in (
                branch_weight,
                conv_state.transpose(1, 0, 2),
                conv_taps,
                decay_logit.reshape(1, half),
            )
        )
    )
    conv_begun, new_state, mixer_in, out_own = pl.pallas_call(
        mixer_body,
        name="mixer",
        out_shape=(
            pltpu.HBM((3, seq_count, half), BF),
            pltpu.HBM((seq_count, half), F32),
            jax.ShapeDtypeStruct((seq_count, half), BF),
            jax.ShapeDtypeStruct((half, half), BF),
        ),
        in_specs=smem() + vmem(10) + hbm(2),
        out_specs=tuple(hbm(2) + vmem(2)),
        scratch_shapes=[
            pltpu.VMEM((features, half), BF),
            pltpu.VMEM((seq_count, half), BF),
            pltpu.VMEM((seq_count, half), F32),
            pltpu.SemaphoreType.DMA((4,)),
        ],
        compiler_params=pltpu.CompilerParams(vmem_limit_bytes=14 * MIB),
        cost_estimate=pl.CostEstimate(
            flops=4 * seq_count * features * half,
            transcendentals=6 * seq_count * half,
            bytes_accessed=4 * features * half,
        ),
    )(
        core_arr,
        stream,
        stream_other,
        mix_gain.reshape(1, features),
        branch_near,
        conv_part,
        conv_taps,
        decay,
        recur_map,
        input_map,
        recur_state,
        in_hbm(gate_weight),
        in_hbm(out_weight),
    )
    own_gate, own_up, own_down, mixer_in = lax.optimization_barrier(
        (own_gate, own_up, own_down, mixer_in)
    )
    mixer_other = swapped(mixer_in)
    other_gate, other_up, other_down = swapped(own_gate), swapped(own_up), swapped(own_down)
    part, out_other = pl.pallas_call(
        near_body,
        name="near",
        out_shape=(
            jax.ShapeDtypeStruct((seq_count, half), F32),
            jax.ShapeDtypeStruct((half, half), BF),
        ),
        in_specs=smem() + vmem(2) + hbm(1),
        out_specs=tuple(vmem(2)),
        scratch_shapes=[pltpu.SemaphoreType.DMA],
        compiler_params=pltpu.CompilerParams(vmem_limit_bytes=8 * MIB),
    )(core_arr, mixer_in, out_own, in_hbm(out_weight))
    resid = pl.pallas_call(
        resid_body,
        name="resid",
        out_shape=jax.ShapeDtypeStruct((seq_count, half), BF),
        in_specs=vmem(4),
        out_specs=vmem(1)[0],
        compiler_params=pltpu.CompilerParams(vmem_limit_bytes=8 * MIB),
    )(part, mixer_other, out_other, stream)
    ids_t, weights_t = route_ids.T, route_weights.T
    count = experts * MAIN
    resid_other = swapped(resid)
    send_table, send_last, table, last = pl.pallas_call(
        route_body,
        name="route",
        out_shape=(
            jax.ShapeDtypeStruct((count, seq_count), BF),
            jax.ShapeDtypeStruct((experts, seq_count), BF),
            jax.ShapeDtypeStruct((2 * seq_count, count), BF),
            jax.ShapeDtypeStruct((2 * seq_count, experts), BF),
        ),
        in_specs=smem() + vmem(2),
        out_specs=tuple(vmem(4)),
        compiler_params=pltpu.CompilerParams(vmem_limit_bytes=8 * MIB),
    )(core_arr, ids_t, weights_t)

    block = features + features // MAIN
    pieces = pltpu.VMEM((2, count, LANES), F32)
    payload, normed_two = pl.pallas_call(
        pack_body,
        name="pack",
        out_shape=(
            jax.ShapeDtypeStruct((count, block), BF),
            jax.ShapeDtypeStruct((seq_count, features), BF),
        ),
        in_specs=smem() + vmem(5),
        out_specs=tuple(vmem(2)),
        scratch_shapes=[pieces],
        compiler_params=pltpu.CompilerParams(vmem_limit_bytes=14 * MIB),
    )(core_arr, resid, resid_other, moe_gain.reshape(1, features), send_table, send_last)

    incoming = lax.all_to_all(
        payload.reshape(experts, MAIN, block), "ep", split_axis=0, concat_axis=0, tiled=True
    )
    incoming, normed_two = lax.optimization_barrier((incoming, normed_two))
    incoming = incoming.reshape(count, block)
    served, dense_hidden, down_near, scale_near, new_conv = pl.pallas_call(
        expert_body,
        name="experts",
        out_shape=(
            jax.ShapeDtypeStruct((count, block), BF),
            jax.ShapeDtypeStruct((seq_count, dense_gate.shape[1]), BF),
            jax.ShapeDtypeStruct(dense_down.shape, BF),
            jax.ShapeDtypeStruct((1, half), F32),
            pltpu.HBM((3, seq_count, half), BF),
        ),
        in_specs=smem() + vmem(11) + hbm(3),
        out_specs=tuple(vmem(4) + hbm(1)),
        input_output_aliases={14: 4},
        scratch_shapes=[
            pieces,
            pieces,
            pltpu.VMEM((experts * SLOTS, features), BF),
            pltpu.SemaphoreType.DMA((3,)),
        ],
        compiler_params=pltpu.CompilerParams(vmem_limit_bytes=20 * MIB),
    )(
        core_arr,
        incoming,
        own_gate,
        other_gate,
        own_up,
        other_up,
        own_down,
        other_down,
        normed_two,
        dense_gate,
        dense_up,
        old_conv,
        in_hbm(dense_down),
        in_hbm(dense_scale.reshape(1, half)),
        in_hbm(conv_begun),
    )
    dense_other = swapped(dense_hidden)
    returned = lax.all_to_all(
        served.reshape(experts, MAIN, block), "ep", split_axis=0, concat_axis=0, tiled=True
    )
    returned = returned.reshape(count, block)
    halves = [pieces, pltpu.VMEM((experts, half), BF)]
    sum_other = pl.pallas_call(
        combine_body,
        name="combine",
        out_shape=jax.ShapeDtypeStruct((seq_count, half), BF),
        in_specs=vmem(3),
        out_specs=vmem(1)[0],
        scratch_shapes=halves,
        compiler_params=pltpu.CompilerParams(vmem_limit_bytes=10 * MIB),
    )(returned, table, last)
    sum_received = swapped(sum_other)
    sum_own = pl.pallas_call(
        finish_body,
        name="finish",
        out_shape=jax.ShapeDtypeStruct((seq_count, half), F32),
        in_specs=smem() + vmem(8),
        out_specs=vmem(1)[0],
        scratch_shapes=halves,
        compiler_params=pltpu.CompilerParams(vmem_limit_bytes=10 * MIB),
    )(
        core_arr,
        returned,
        table,
        last,
        resid,
        dense_hidden,
        dense_other,
        down_near,
        scale_near,
    )
    result = (sum_own + sum_received.astype(F32)).astype(BF)
    new_conv = new_conv.transpose(1, 0, 2)
    return (result, new_state, new_conv)


def solution(mesh):
    in_specs = (
        P("ep", "tp"),
        P("ep", None, "tp"),
        P("ep", "tp"),
        P(),
        P(None, "tp"),
        P(None, "tp"),
        P(None, "tp"),
        P("tp", None, None),
        P("tp", None, None),
        P("tp"),
        P(None, "tp"),
        P(),
        P("ep", None),
        P("ep", None),
        P("ep", None, "tp"),
        P("ep", None, "tp"),
        P("ep", None, "tp"),
        P(None, "tp"),
        P(None, "tp"),
        P(None, "tp"),
        P("tp"),
    )
    out_specs = (P("ep", "tp"), P("ep", "tp"), P("ep", None, "tp"))
    return jax.shard_map(
        per_device, mesh=mesh, in_specs=in_specs, out_specs=out_specs, check_vma=False
    )
```

```python
import functools

import jax
import jax.numpy as jnp
from jax import lax
from jax.experimental import pallas as pl
from jax.experimental.pallas import tpu as pltpu
from jax.sharding import PartitionSpec as P


BF = jnp.bfloat16
F32 = jnp.float32
SWAP = [(0, 1), (1, 0)]
MIB = 1024 * 1024
LANES = 128
SLOTS = 9
MAIN = 8


def swapped(x):
    return lax.ppermute(x, "tp", SWAP)


def places(ids, core):
    experts = rows = ids.shape[1]
    expert = lax.broadcasted_iota(jnp.int32, (experts, rows), 0)
    hits = [ids[k : k + 1, :] == expert for k in range(ids.shape[0])]
    chosen = functools.reduce(jnp.logical_or, hits)
    earlier = lax.broadcasted_iota(jnp.int32, (rows, rows), 0) < lax.broadcasted_iota(
        jnp.int32, (rows, rows), 1
    )
    rank = jnp.dot(
        jnp.where(chosen, 1.0, 0.0).astype(BF),
        jnp.where(earlier, 1.0, 0.0).astype(BF),
        preferred_element_type=F32,
    )
    return hits, jnp.where(chosen, rank - (SLOTS * core).astype(F32), -1.0)


def each_slot(values):
    experts = values.shape[0]
    shape = (experts * MAIN, experts)
    row = lax.broadcasted_iota(jnp.int32, shape, 0) // MAIN
    spread = jnp.where(row == lax.broadcasted_iota(jnp.int32, shape, 1), 1.0, 0.0).astype(BF)
    return jnp.dot(spread, values.astype(BF), preferred_element_type=F32)


def slot_number(shape):
    return (lax.broadcasted_iota(jnp.int32, shape, 0) % MAIN).astype(F32)


def put_pieces(piece_ref, values, start, base):
    count = values.shape[0]
    for n in range(values.shape[1] // LANES):
        c, part = divmod(start + n, 2)
        piece_ref[part, pl.ds(base + c, count, stride=MAIN), :] = values[
            :, n * LANES : (n + 1) * LANES
        ]


def take_pieces(piece_ref, block_ref, features, rows_ref, low=0, high=None):
    count = block_ref.shape[0] // MAIN
    piece_ref[0] = block_ref[:, features : features + LANES].astype(F32)
    piece_ref[1] = block_ref[:, features + LANES :].astype(F32)
    for n in range(low // LANES, (high or features) // LANES):
        c, part = divmod(n, 2)
        column = n * LANES - low
        rows_ref[:count, column : column + LANES] = piece_ref[
            part, pl.ds(c, count, stride=MAIN), :
        ].astype(BF)


def route_body(
    core_ref, ids_ref, weights_ref, table_ref, last_ref, back_table_ref, back_last_ref
):
    rows = ids_ref.shape[1]
    hits, place = places(ids_ref[...], core_ref[0])
    wide = each_slot(place)
    match = wide == slot_number(wide.shape)
    table_ref[...] = jnp.where(match, 1.0, 0.0).astype(BF)
    last_ref[...] = jnp.where(place == float(MAIN), 1.0, 0.0).astype(BF)
    weight = functools.reduce(
        jnp.add,
        [jnp.where(hit, weights_ref[k : k + 1, :], 0.0) for k, hit in enumerate(hits)],
    )
    high = weight.astype(BF).astype(F32)
    low = (weight - high).astype(BF).astype(F32)
    for n, part in enumerate((high, low)):
        span = slice(n * rows, (n + 1) * rows)
        back_table_ref[span, :] = jnp.transpose(jnp.where(match, each_slot(part), 0.0)).astype(BF)
        back_last_ref[span, :] = jnp.transpose(
            jnp.where(place == float(MAIN), part, 0.0)
        ).astype(BF)


def pack_body(
    core_ref,
    own_ref,
    other_ref,
    gain_ref,
    table_ref,
    last_ref,
    out_ref,
    norm_ref,
    piece_ref,
):
    core = core_ref[0]
    half = own_ref.shape[1]
    features = 2 * half
    own = own_ref[...].astype(F32)
    other = other_ref[...].astype(F32)
    mean = (jnp.sum(own, 1, keepdims=True) + jnp.sum(other, 1, keepdims=True)) / features
    square = (
        jnp.sum(own * own, 1, keepdims=True) + jnp.sum(other * other, 1, keepdims=True)
    ) / features
    scale = lax.rsqrt(square - mean * mean + 1e-05)
    low, high = gain_ref[:, :half], gain_ref[:, half:]
    gain_own = jnp.where(core == 0, low, high)
    gain_other = jnp.where(core == 0, high, low)
    norm_ref[:, :half] = ((own - mean) * scale * gain_own).astype(BF)
    norm_ref[:, half:] = ((other - mean) * scale * gain_other).astype(BF)
    rows = norm_ref[...]
    put_pieces(piece_ref, jnp.dot(last_ref[...], rows, preferred_element_type=F32), 0, 0)
    out_ref[:, :features] = jnp.dot(table_ref[...], rows, preferred_element_type=F32).astype(BF)
    out_ref[:, features : features + LANES] = piece_ref[0].astype(BF)
    out_ref[:, features + LANES :] = piece_ref[1].astype(BF)


def start_all(pairs, sems):
    copies = [
        pltpu.make_async_copy(source, target, sems.at[n])
        for n, (source, target) in enumerate(pairs)
    ]
    for copy in copies:
        copy.start()
    return copies


def wait_all(copies):
    for copy in copies:
        copy.wait()


def warm_body(
    weight_hbm,
    state_hbm,
    taps_hbm,
    logit_hbm,
    weight_ref,
    conv_ref,
    decay_ref,
    state_ref,
    taps_ref,
    logit_ref,
    sems,
):
    copies = start_all(
        (
            (state_hbm, state_ref),
            (taps_hbm, taps_ref),
            (logit_hbm, logit_ref),
            (weight_hbm, weight_ref),
        ),
        sems,
    )
    wait_all(copies[:3])
    conv = state_ref[0].astype(F32) * taps_ref[0:1, :]
    for offset in range(1, 3):
        conv = conv + state_ref[offset].astype(F32) * taps_ref[offset : offset + 1, :]
    conv_ref[...] = conv
    decay_ref[...] = -8.0 * jax.nn.softplus(-logit_ref[...])
    wait_all(copies[3:])


def near_body(core_ref, mixed_ref, weight_ref, weight_hbm, part_ref, other_ref, sem):
    half = mixed_ref.shape[1]
    second = pl.ds(pl.multiple_of((1 - core_ref[0]) * half, half), half)
    copy = pltpu.make_async_copy(weight_hbm.at[second, :], other_ref, sem)
    copy.start()
    part_ref[...] = jnp.dot(mixed_ref[...], weight_ref[...], preferred_element_type=F32)
    copy.wait()


def resid_body(part_ref, mixed_ref, weight_ref, stream_ref, out_ref):
    mixer_out = part_ref[...] + jnp.dot(
        mixed_ref[...], weight_ref[...], preferred_element_type=F32
    )
    out_ref[...] = (stream_ref[...].astype(F32) + mixer_out.astype(BF).astype(F32)).astype(BF)


def mixer_body(
    core_ref,
    own_ref,
    other_ref,
    gain_ref,
    branch_ref,
    conv_ref,
    taps_ref,
    decay_ref,
    recur_ref,
    input_ref,
    state_ref,
    gate_hbm,
    out_hbm,
    new_conv_hbm,
    new_state_hbm,
    mixed_ref,
    weight_ref,
    gate_ref,
    branch_out_ref,
    state_out_ref,
    sems,
):
    core = core_ref[0]
    half = own_ref.shape[1]
    features = 2 * half
    first = pl.ds(pl.multiple_of(core * half, half), half)
    second = pl.ds(pl.multiple_of((1 - core) * half, half), half)
    gate_copy = pltpu.make_async_copy(gate_hbm, gate_ref, sems.at[0])
    gate_copy.start()
    out_copy = pltpu.make_async_copy(out_hbm.at[first, :], weight_ref, sems.at[1])
    own = own_ref[...].astype(F32)
    other = other_ref[...].astype(F32)
    mean = (jnp.sum(own, 1, keepdims=True) + jnp.sum(other, 1, keepdims=True)) / features
    square = (
        jnp.sum(own * own, 1, keepdims=True) + jnp.sum(other * other, 1, keepdims=True)
    ) / features
    scale = lax.rsqrt(square - mean * mean + 1e-05)
    low, high = gain_ref[:, :half], gain_ref[:, half:]
    own = ((own - mean) * scale * jnp.where(core == 0, low, high)).astype(BF)
    other = ((other - mean) * scale * jnp.where(core == 0, high, low)).astype(BF)

    def product(weight):
        return (
            jnp.dot(own, weight[first, :], preferred_element_type=F32)
            + jnp.dot(other, weight[second, :], preferred_element_type=F32)
        ).astype(BF)

    branch = product(branch_ref)
    out_copy.start()
    branch_out_ref[...] = branch
    conv = (conv_ref[...] + branch.astype(F32) * taps_ref[3:4, :]).astype(BF)
    width = recur_ref.shape[1]
    recur, drive = (
        jnp.concatenate(
            [
                jnp.dot(
                    conv[:, n * width : (n + 1) * width], maps[n], preferred_element_type=F32
                )
                for n in range(maps.shape[0])
            ],
            axis=1,
        )
        for maps in (recur_ref, input_ref)
    )
    log_decay = jax.nn.sigmoid(recur) * decay_ref[...]
    turn = jnp.tanh(log_decay)
    kept = jnp.sqrt(-2.0 * turn / (1.0 - turn))
    driven = kept * (jax.nn.sigmoid(drive) * conv.astype(F32))
    state = jnp.exp(log_decay) * state_ref[...] + driven
    state_out_ref[...] = state
    branch_copy = pltpu.make_async_copy(branch_out_ref, new_conv_hbm.at[2], sems.at[2])
    branch_copy.start()
    state_copy = pltpu.make_async_copy(state_out_ref, new_state_hbm, sems.at[3])
    state_copy.start()
    gate_copy.wait()
    mixed_ref[...] = (jax.nn.gelu(product(gate_ref).astype(F32)) * state).astype(BF)
    wait_all([out_copy, branch_copy, state_copy])


def expert_body(
    core_ref,
    in_ref,
    gate_ref,
    gate2_ref,
    up_ref,
    up2_ref,
    down_ref,
    down2_ref,
    normed_ref,
    dense_gate_ref,
    dense_up_ref,
    old_conv_ref,
    dense_down_hbm,
    dense_scale_hbm,
    conv_begun_hbm,
    out_ref,
    dense_ref,
    dense_down_ref,
    dense_scale_ref,
    new_conv_hbm,
    piece_ref,
    take_ref,
    rows_ref,
    sems,
):
    copies = start_all(
        (
            (dense_down_hbm, dense_down_ref),
            (dense_scale_hbm, dense_scale_ref),
            (old_conv_ref.at[pl.ds(1, 2)], new_conv_hbm.at[pl.ds(0, 2)]),
        ),
        sems,
    )
    core = core_ref[0]
    features, units = gate_ref.shape
    half = features // 2
    first = pl.ds(pl.multiple_of(core * half, half), half)
    second = pl.ds(pl.multiple_of((1 - core) * half, half), half)
    unit_own = pl.ds(pl.multiple_of(core * units, units), units)
    unit_other = pl.ds(pl.multiple_of((1 - core) * units, units), units)
    count = in_ref.shape[0]
    extra = count // MAIN
    take_pieces(take_ref, in_ref, features, rows_ref)
    rows_ref[extra:, :] = in_ref[:, :features]

    def hidden(rows, gate, up):
        gated, raised = (
            jnp.dot(rows[:, :half], weight[first, :], preferred_element_type=F32)
            + jnp.dot(rows[:, half:], weight[second, :], preferred_element_type=F32)
            for weight in (gate, up)
        )
        return (jax.nn.silu(gated) * raised).astype(BF)

    dense_ref[...] = hidden(normed_ref, dense_gate_ref, dense_up_ref)
    hid_own = hidden(rows_ref, gate_ref, up_ref)
    hid_other = hidden(rows_ref, gate2_ref, up2_ref)

    def served(down, span):
        return jnp.dot(hid_own[span], down[unit_own, :], preferred_element_type=F32) + jnp.dot(
            hid_other[span], down[unit_other, :], preferred_element_type=F32
        )

    for part, down in enumerate((down_ref, down2_ref)):
        values = served(down, slice(None))
        put_pieces(piece_ref, values[:extra], part * (half // LANES), 0)
        out_ref[:, part * half : (part + 1) * half] = values[extra:].astype(BF)
    out_ref[:, features : features + LANES] = piece_ref[0].astype(BF)
    out_ref[:, features + LANES :] = piece_ref[1].astype(BF)
    wait_all(copies)


def half_sum(in_ref, table_ref, lasts_ref, piece_ref, last_ref, low, high, features):
    take_pieces(piece_ref, in_ref, features, last_ref, low, high)
    total = jnp.dot(
        table_ref[...], in_ref[:, low:high], preferred_element_type=F32
    ) + jnp.dot(lasts_ref[...], last_ref[...], preferred_element_type=F32)
    rows = total.shape[0] // 2
    return total[:rows] + total[rows:]


def combine_body(in_ref, table_ref, lasts_ref, other_ref, piece_ref, last_ref):
    half = other_ref.shape[1]
    other_ref[...] = half_sum(
        in_ref, table_ref, lasts_ref, piece_ref, last_ref, half, 2 * half, 2 * half
    ).astype(BF)


def finish_body(
    core_ref,
    in_ref,
    table_ref,
    lasts_ref,
    resid_ref,
    own_hid_ref,
    other_hid_ref,
    down_ref,
    scale_ref,
    own_ref,
    piece_ref,
    last_ref,
):
    core = core_ref[0]
    half = own_ref.shape[1]
    units = own_hid_ref.shape[1]
    unit_own = pl.ds(pl.multiple_of(core * units, units), units)
    unit_other = pl.ds(pl.multiple_of((1 - core) * units, units), units)
    dense = jnp.dot(own_hid_ref[...], down_ref[unit_own, :], preferred_element_type=F32) + jnp.dot(
        other_hid_ref[...], down_ref[unit_other, :], preferred_element_type=F32
    )
    base = resid_ref[...].astype(F32) + scale_ref[...] * dense.astype(BF).astype(F32)
    own_ref[...] = base + half_sum(
        in_ref, table_ref, lasts_ref, piece_ref, last_ref, 0, half, 2 * half
    )


def vmem(count):
    return [pl.BlockSpec(memory_space=pltpu.VMEM)] * count


def hbm(count):
    return [pl.BlockSpec(memory_space=pltpu.HBM)] * count


def in_hbm(x):
    return pltpu.with_memory_space_constraint(x, pltpu.HBM)


def smem():
    return [pl.BlockSpec(memory_space=pltpu.SMEM)]


def per_device(
    stream,
    conv_state,
    recur_state,
    mix_gain,
    branch_weight,
    gate_weight,
    conv_taps,
    recur_map,
    input_map,
    decay_logit,
    out_weight,
    moe_gain,
    route_ids,
    route_weights,
    expert_gate,
    expert_up,
    expert_down,
    dense_gate,
    dense_up,
    dense_down,
    dense_scale,
):
    core = lax.axis_index("tp")
    core_arr = core.astype(jnp.int32).reshape(1)
    seq_count, half = stream.shape
    features = 2 * half
    experts = lax.axis_size("ep")
    own_gate, own_up, own_down = expert_gate[0], expert_up[0], expert_down[0]
    stream_other = swapped(stream)
    branch_near, conv_part, decay, old_conv = pl.pallas_call(
        warm_body,
        name="warm",
        out_shape=(
            jax.ShapeDtypeStruct((features, half), BF),
            jax.ShapeDtypeStruct((seq_count, half), F32),
            jax.ShapeDtypeStruct((1, half), F32),
            jax.ShapeDtypeStruct((3, seq_count, half), BF),
        ),
        in_specs=hbm(4),
        out_specs=tuple(vmem(4)),
        scratch_shapes=[
            pltpu.VMEM((4, half), F32),
            pltpu.VMEM((1, half), F32),
            pltpu.SemaphoreType.DMA((4,)),
        ],
        compiler_params=pltpu.CompilerParams(vmem_limit_bytes=8 * MIB),
    )(
        *(
            in_hbm(x)
            for x in (
                branch_weight,
                conv_state.transpose(1, 0, 2),
                conv_taps,
                decay_logit.reshape(1, half),
            )
        )
    )
    conv_begun, new_state, mixer_in, out_own = pl.pallas_call(
        mixer_body,
        name="mixer",
        out_shape=(
            pltpu.HBM((3, seq_count, half), BF),
            pltpu.HBM((seq_count, half), F32),
            jax.ShapeDtypeStruct((seq_count, half), BF),
            jax.ShapeDtypeStruct((half, half), BF),
        ),
        in_specs=smem() + vmem(10) + hbm(2),
        out_specs=tuple(hbm(2) + vmem(2)),
        scratch_shapes=[
            pltpu.VMEM((features, half), BF),
            pltpu.VMEM((seq_count, half), BF),
            pltpu.VMEM((seq_count, half), F32),
            pltpu.SemaphoreType.DMA((4,)),
        ],
        compiler_params=pltpu.CompilerParams(vmem_limit_bytes=14 * MIB),
        cost_estimate=pl.CostEstimate(
            flops=4 * seq_count * features * half,
            transcendentals=6 * seq_count * half,
            bytes_accessed=4 * features * half,
        ),
    )(
        core_arr,
        stream,
        stream_other,
        mix_gain.reshape(1, features),
        branch_near,
        conv_part,
        conv_taps,
        decay,
        recur_map,
        input_map,
        recur_state,
        in_hbm(gate_weight),
        in_hbm(out_weight),
    )
    own_gate, own_up, own_down, mixer_in = lax.optimization_barrier(
        (own_gate, own_up, own_down, mixer_in)
    )
    mixer_other = swapped(mixer_in)
    other_gate, other_up, other_down = swapped(own_gate), swapped(own_up), swapped(own_down)
    part, out_other = pl.pallas_call(
        near_body,
        name="near",
        out_shape=(
            jax.ShapeDtypeStruct((seq_count, half), F32),
            jax.ShapeDtypeStruct((half, half), BF),
        ),
        in_specs=smem() + vmem(2) + hbm(1),
        out_specs=tuple(vmem(2)),
        scratch_shapes=[pltpu.SemaphoreType.DMA],
        compiler_params=pltpu.CompilerParams(vmem_limit_bytes=8 * MIB),
    )(core_arr, mixer_in, out_own, in_hbm(out_weight))
    resid = pl.pallas_call(
        resid_body,
        name="resid",
        out_shape=jax.ShapeDtypeStruct((seq_count, half), BF),
        in_specs=vmem(4),
        out_specs=vmem(1)[0],
        compiler_params=pltpu.CompilerParams(vmem_limit_bytes=8 * MIB),
    )(part, mixer_other, out_other, stream)
    ids_t, weights_t = route_ids.T, route_weights.T
    count = experts * MAIN
    resid_other = swapped(resid)
    send_table, send_last, table, last = pl.pallas_call(
        route_body,
        name="route",
        out_shape=(
            jax.ShapeDtypeStruct((count, seq_count), BF),
            jax.ShapeDtypeStruct((experts, seq_count), BF),
            jax.ShapeDtypeStruct((2 * seq_count, count), BF),
            jax.ShapeDtypeStruct((2 * seq_count, experts), BF),
        ),
        in_specs=smem() + vmem(2),
        out_specs=tuple(vmem(4)),
        compiler_params=pltpu.CompilerParams(vmem_limit_bytes=8 * MIB),
    )(core_arr, ids_t, weights_t)

    block = features + features // MAIN
    pieces = pltpu.VMEM((2, count, LANES), F32)
    payload, normed_two = pl.pallas_call(
        pack_body,
        name="pack",
        out_shape=(
            jax.ShapeDtypeStruct((count, block), BF),
            jax.ShapeDtypeStruct((seq_count, features), BF),
        ),
        in_specs=smem() + vmem(5),
        out_specs=tuple(vmem(2)),
        scratch_shapes=[pieces],
        compiler_params=pltpu.CompilerParams(vmem_limit_bytes=14 * MIB),
    )(core_arr, resid, resid_other, moe_gain.reshape(1, features), send_table, send_last)

    incoming = lax.all_to_all(
        payload.reshape(experts, MAIN, block), "ep", split_axis=0, concat_axis=0, tiled=True
    )
    incoming, normed_two = lax.optimization_barrier((incoming, normed_two))
    incoming = incoming.reshape(count, block)
    served, dense_hidden, down_near, scale_near, new_conv = pl.pallas_call(
        expert_body,
        name="experts",
        out_shape=(
            jax.ShapeDtypeStruct((count, block), BF),
            jax.ShapeDtypeStruct((seq_count, dense_gate.shape[1]), BF),
            jax.ShapeDtypeStruct(dense_down.shape, BF),
            jax.ShapeDtypeStruct((1, half), F32),
            pltpu.HBM((3, seq_count, half), BF),
        ),
        in_specs=smem() + vmem(11) + hbm(3),
        out_specs=tuple(vmem(4) + hbm(1)),
        input_output_aliases={14: 4},
        scratch_shapes=[
            pieces,
            pieces,
            pltpu.VMEM((experts * SLOTS, features), BF),
            pltpu.SemaphoreType.DMA((3,)),
        ],
        compiler_params=pltpu.CompilerParams(vmem_limit_bytes=20 * MIB),
    )(
        core_arr,
        incoming,
        own_gate,
        other_gate,
        own_up,
        other_up,
        own_down,
        other_down,
        normed_two,
        dense_gate,
        dense_up,
        old_conv,
        in_hbm(dense_down),
        in_hbm(dense_scale.reshape(1, half)),
        in_hbm(conv_begun),
    )
    dense_other = swapped(dense_hidden)
    returned = lax.all_to_all(
        served.reshape(experts, MAIN, block), "ep", split_axis=0, concat_axis=0, tiled=True
    )
    returned = returned.reshape(count, block)
    halves = [pieces, pltpu.VMEM((experts, half), BF)]
    sum_other = pl.pallas_call(
        combine_body,
        name="combine",
        out_shape=jax.ShapeDtypeStruct((seq_count, half), BF),
        in_specs=vmem(3),
        out_specs=vmem(1)[0],
        scratch_shapes=halves,
        compiler_params=pltpu.CompilerParams(vmem_limit_bytes=10 * MIB),
    )(returned, table, last)
    sum_received = swapped(sum_other)
    sum_own = pl.pallas_call(
        finish_body,
        name="finish",
        out_shape=jax.ShapeDtypeStruct((seq_count, half), F32),
        in_specs=smem() + vmem(8),
        out_specs=vmem(1)[0],
        scratch_shapes=halves,
        compiler_params=pltpu.CompilerParams(vmem_limit_bytes=10 * MIB),
    )(
        core_arr,
        returned,
        table,
        last,
        resid,
        dense_hidden,
        dense_other,
        down_near,
        scale_near,
    )
    result = (sum_own + sum_received.astype(F32)).astype(BF)
    new_conv = new_conv.transpose(1, 0, 2)
    return (result, new_state, new_conv)


def solution(mesh):
    in_specs = (
        P("ep", "tp"),
        P("ep", None, "tp"),
        P("ep", "tp"),
        P(),
        P(None, "tp"),
        P(None, "tp"),
        P(None, "tp"),
        P("tp", None, None),
        P("tp", None, None),
        P("tp"),
        P(None, "tp"),
        P(),
        P("ep", None),
        P("ep", None),
        P("ep", None, "tp"),
        P("ep", None, "tp"),
        P("ep", None, "tp"),
        P(None, "tp"),
        P(None, "tp"),
        P(None, "tp"),
        P("tp"),
    )
    out_specs = (P("ep", "tp"), P("ep", "tp"), P("ep", None, "tp"))
    return jax.shard_map(
        per_device, mesh=mesh, in_specs=in_specs, out_specs=out_specs, check_vma=False
    )
```
